512 devices in a mesh: grp: 2 (over y), ep: 32 (over z, core), tp: 8 (over x).
Axes of the slice: x: 8, y: 2, z: 16, core: 2. Of those that a mesh axis runs over, the one named last changes fastest.
The devices are a block of a 8x8x16 slice.
Arguments:
- queries: bfloat16 [8192, 1024], P(('grp', 'ep'), 'tp'), parts along dimension 0, may hold values from -6 to 6
- keys: bfloat16 [8192, 1024], P(('grp', 'ep'), 'tp'), parts along dimension 0, may hold values from -6 to 6
- values: bfloat16 [8192, 1024], P(('grp', 'ep'), 'tp'), parts along dimension 0, may hold values from -6 to 6
- lambdas: float32 [8], P('tp'), may hold values from 0.3 to 0.8
- head_gain: float32 [128], replicated, may hold values from 0.1 to 1.9
- tokens: bfloat16 [16384, 1536], P(('grp', 'ep')), parts along dimension 0, may hold values from -6 to 6
- route_ids: int32 [16384, 2], P(('grp', 'ep')), parts along dimension 0, may hold values from 0 to 31, all different within a row; in each aligned block of 256 rows (0 to 255, 256 to 511, ...) at most 32 rows name the same one
- route_weights: float32 [16384, 2], P(('grp', 'ep')), parts along dimension 0, may hold values from 0.2 to 1
- moe_gain: float32 [1536], replicated, may hold values from 0.1 to 1.9
- w_gate: bfloat16 [32, 1536, 3072], P('ep', None, 'tp'), may hold values from -0.15625 to 0.15625
- w_up: bfloat16 [32, 1536, 3072], P('ep', None, 'tp'), may hold values from -0.15625 to 0.15625
- w_down: bfloat16 [32, 3072, 1536], P('ep', 'tp'), may hold values from -0.109375 to 0.109375
Outputs:
- heads_out: bfloat16 [8192, 1024], P(('grp', 'ep'), 'tp'), parts along dimension 0
- expert_out: bfloat16 [16384, 1536], P(('grp', 'ep'), 'tp'), parts along dimension 0
The draws below stay inside these ranges and needn't reach their ends.
There are 2 independent parts, one for each index of `grp`. The reference program is written for one: setup_inputs(seed, part) draws one part's arguments, and reference() takes and returns one part's arrays. A program takes and returns all parts, laid end to end along the dimension named above; an argument that names none is the same for every part. Nothing has to cross between parts.
Inputs may be any that keep to these rules, and one draw needn't show every extreme that they name: `route_ids`: each row names 2 different experts. In the 256 rows of one device no expert is named more than 32 times, and in every draw some device names some expert exactly 32 times.
All inputs are finite; a program needn't handle non-finite values.
Results may differ from the reference program's by a relative error of at most 0.015.
Values may be sent and summed in bfloat16 or wider, within the bound.
A program may use at most 64 MiB of HBM per device.

```python
import math
import jax
import jax.numpy as jnp
import numpy as np
from jax import lax

D = 1536
FF = 3072
HEADS = 8
HEAD_DIM = 64
VALUE_DIM = 128
TOP = 2
ROW_DEV = 256
EXPERTS = 32
CAP = 32
SEQ = 4096
ROWS = 8192
N_EP = 32
N_TP = 8


def draw_pair(key):
    base = jax.random.fold_in(key, 17)
    width = HEADS * 2 * HEAD_DIM
    query_key, key_key = jax.random.split(base, 2)
    query_field = jnp.clip(jax.random.normal(query_key, (SEQ, width), jnp.float32) * 1.33, -6.0, 6.0)
    key_field = jnp.clip(jax.random.normal(key_key, (SEQ, width), jnp.float32) * 1.33, -6.0, 6.0)
    return (query_field, key_field)


def draw_queries(key, part):
    return draw_pair(key)[0].astype(jnp.bfloat16)


def draw_keys(key, part):
    return draw_pair(key)[1].astype(jnp.bfloat16)


def block_scale(own_key, extent, pieces, smallest, largest):
    factor_of = 1.0
    for dim, blocks in pieces:
        heights = jax.random.uniform(jax.random.fold_in(jax.random.fold_in(own_key, 6), dim), (blocks,), jnp.float32, smallest / len(pieces), largest / len(pieces))
        factor_of = factor_of * jnp.repeat(jnp.exp(heights), extent[dim] // blocks).reshape((-1,) + (1,) * (len(extent) - 1 - dim))
    return factor_of


def deal_out(own_key, own, number, rows, amount, top, most, slope):
    ranking = jax.random.permutation(own_key, amount)
    heavy_load, usual = shares(amount, rows * top, most, slope, True), shares(amount, rows * top, most, slope, False)
    places = jnp.arange(amount)

    def named(sizes, offset_by):
        used = int((sizes > 0).sum())
        fixed = max(1, used // 4)
        moved = fixed + (places - fixed + offset_by * (used - fixed)) % max(1, amount - fixed)
        return jnp.zeros((amount,), jnp.int32).at[ranking[jnp.where(places < fixed, places, moved)]].set(jnp.asarray(sizes, jnp.int32))

    sizes = jnp.where(number % 4 == 0, named(heavy_load, number // 4), named(usual, number - number // 4 - 1))
    mixed = jax.random.permutation(jax.random.fold_in(own, 3), amount)
    source_of, sink = mixed[0:amount // 2 * 2:2], mixed[1:amount // 2 * 2:2]
    margin = jnp.minimum(sizes[source_of] - 1, most - sizes[sink]) // 2
    margin = jnp.where((source_of == ranking[0]) | (sink == ranking[0]) | (sizes[sink] == 0), 0, jnp.maximum(margin, 0))
    moved = jax.random.randint(jax.random.fold_in(own, 4), (amount // 2,), 0, 1 << 20) % (margin + 1)
    sizes = sizes.at[source_of].add(-moved).at[sink].add(moved)
    items = jnp.searchsorted(jnp.cumsum(sizes), jnp.arange(rows * top), side="right").astype(jnp.int32)
    listing = items.reshape(top, rows).T
    listing = listing[jax.random.permutation(jax.random.fold_in(own, 1), rows)]
    offset_by = jax.random.randint(jax.random.fold_in(own, 2), (rows, 1), 0, top)
    return jnp.take_along_axis(listing, (jnp.arange(top)[None, :] + offset_by) % top, axis=1)


def shares(count, total, bound, slope, full):
    weights = [(1 << 20) // math.isqrt(rank ** slope) + 1 for rank in range(1, count + 1)]
    largest = bound if full else min(bound, max(-(-total // count), total * weights[0] // sum(weights)))
    least = 1 if total - largest >= count - 1 else 0
    counts, surplus = [largest] + [least] * (count - 1), total - largest - least * (count - 1)
    while surplus > 0:
        free = [i for i in range(1, count) if counts[i] < largest] or [i for i in range(1, count) if counts[i] < bound]
        mass, budget = sum([weights[i] for i in free]), surplus
        for i in free:
            more = min(bound - counts[i], max(1, budget * weights[i] // mass), surplus)
            counts[i] = counts[i] + more
            surplus = surplus - more
    return np.array(counts)


def bell_draw(key, dims, spread, limit, shards=(), kind=jnp.bfloat16):
    factor_of = block_scale(key, dims, shards, -0.22, 0.18) if shards else 1.0
    entries = jax.random.normal(key, dims, jnp.float32) * spread * factor_of
    return jnp.minimum(jnp.maximum(entries, -limit), limit).astype(kind)


def setup_inputs(seed: int = 0, part: int = 0) -> dict:
    splits = jax.random.split(jax.random.key(seed), 13)
    own_keys = jax.random.split(jax.random.fold_in(splits[12], part), 13)
    queries = draw_queries(jax.random.fold_in(jax.random.fold_in(splits[12], part), 71), part)
    keys = draw_keys(jax.random.fold_in(jax.random.fold_in(splits[12], part), 71), part)
    values = bell_draw(own_keys[2], (SEQ, HEADS * VALUE_DIM), 1.0, 6.0, ((0, 32), (1, 8)))
    lambdas = jnp.clip(0.3 + 0.5 * jax.random.uniform(splits[3], (HEADS,), jnp.float32) ** block_scale(splits[3], (HEADS,), ((0, 8),), -0.2, 0.2), 0.3, 0.8)
    head_gain = jnp.clip(1.0 + 0.18 * jax.random.normal(splits[4], (VALUE_DIM,), jnp.float32), 0.1, 1.9)
    tokens = bell_draw(own_keys[5], (ROWS, D), 1.0, 6.0, ((0, 32),))
    route_ids_keys = jax.random.split(jax.random.fold_in(own_keys[6], 1), ROWS // ROW_DEV)
    route_ids_turns = jax.random.permutation(jax.random.fold_in(own_keys[6], 3), ROWS // ROW_DEV)
    route_ids = jax.vmap(lambda own, number: deal_out(jax.random.fold_in(own_keys[6], 2), own, number, ROW_DEV, EXPERTS, TOP, CAP, 2))(route_ids_keys, route_ids_turns).reshape((ROWS, TOP))
    route_weights = jnp.clip(0.2 + 0.8 * jax.random.uniform(own_keys[7], (ROWS, TOP), jnp.float32) ** block_scale(own_keys[7], (ROWS, TOP), ((0, 32),), -0.2, 0.2), 0.2, 1.0)
    moe_gain = jnp.clip(1.0 + 0.18 * jax.random.normal(splits[8], (D,), jnp.float32), 0.1, 1.9)
    w_gate = bell_draw(splits[9], (EXPERTS, D, FF), D ** -0.5, 0.15625, ((0, 32), (2, 8)))
    w_up = bell_draw(splits[10], (EXPERTS, D, FF), D ** -0.5, 0.15625, ((0, 32), (2, 8)))
    w_down = bell_draw(splits[11], (EXPERTS, FF, D), FF ** -0.5, 0.109375, ((0, 32), (1, 8)))
    return dict(queries=queries, keys=keys, values=values, lambdas=lambdas, head_gain=head_gain, tokens=tokens, route_ids=route_ids, route_weights=route_weights, moe_gain=moe_gain, w_gate=w_gate, w_up=w_up, w_down=w_down)


def head_mix(operands):
    query_head, key_head, value_head, lambda_head, head_gain = operands
    block = math.gcd(SEQ, 512)
    query_blocks = query_head.reshape(SEQ // block, block, 2, HEAD_DIM)

    def one_block(query_part):
        results = []
        for component in range(2):
            scores = jnp.dot(query_part[:, component], key_head[:, component].T, preferred_element_type=jnp.float32) * HEAD_DIM ** (-0.5)
            highest = lax.optimization_barrier(jnp.max(scores, axis=1, keepdims=True))
            shifted = jnp.exp(scores - highest)
            totals = lax.optimization_barrier(jnp.sum(shifted, axis=1, keepdims=True))
            sums = jnp.dot(shifted.astype(jnp.bfloat16), value_head, preferred_element_type=jnp.float32)
            results.append(sums / totals)
        mixed = results[0] - lambda_head * results[1]
        scaled = mixed * lax.rsqrt(lax.optimization_barrier(jnp.mean(mixed * mixed, axis=1, keepdims=True)) + 1e-06) * head_gain
        return scaled.astype(jnp.bfloat16)
    return lax.map(one_block, query_blocks).reshape(SEQ, VALUE_DIM)

def reference(queries, keys, values, lambdas, head_gain, tokens, route_ids, route_weights, moe_gain, w_gate, w_up, w_down):
    query_heads = jnp.transpose(queries.reshape(SEQ, HEADS, 2, HEAD_DIM), (1, 0, 2, 3))
    key_heads = jnp.transpose(keys.reshape(SEQ, HEADS, 2, HEAD_DIM), (1, 0, 2, 3))
    value_heads = jnp.transpose(values.reshape(SEQ, HEADS, VALUE_DIM), (1, 0, 2))
    gains = jnp.broadcast_to(head_gain, (HEADS, VALUE_DIM))
    mixed_heads = lax.map(head_mix, (query_heads, key_heads, value_heads, lambdas, gains))
    heads_out = jnp.transpose(mixed_heads, (1, 0, 2)).reshape(SEQ, HEADS * VALUE_DIM)
    token_float = tokens.astype(jnp.float32)
    normed = (token_float * lax.rsqrt(lax.optimization_barrier(jnp.mean(token_float * token_float, axis=1, keepdims=True)) + 1e-06) * moe_gain).astype(jnp.bfloat16)
    flat_ids = route_ids.reshape(N_EP, ROW_DEV * TOP)
    onehot = (flat_ids[:, :, None] == jnp.arange(EXPERTS, dtype=jnp.int32)[None, None, :]).astype(jnp.int32)
    earlier = jnp.cumsum(onehot, axis=1) - onehot
    position = lax.optimization_barrier(jnp.sum(earlier * onehot, axis=2)).astype(jnp.int32)
    source = jnp.broadcast_to(jnp.arange(N_EP, dtype=jnp.int32)[:, None], (N_EP, ROW_DEV * TOP))
    owner_row = source * ROW_DEV + jnp.arange(ROW_DEV * TOP, dtype=jnp.int32)[None, :] // TOP
    table = jnp.full((EXPERTS, N_EP, CAP), ROWS, jnp.int32).at[flat_ids, source, position].set(owner_row)
    padded = jnp.concatenate([normed, jnp.zeros((1, D), jnp.bfloat16)], axis=0)

    def expert_pass(operands):
        rows_index, gate_mat, up_mat, down_mat = operands
        arrived = padded[rows_index.reshape(-1)]
        gate = jnp.dot(arrived, gate_mat, preferred_element_type=jnp.float32)
        upward = jnp.dot(arrived, up_mat, preferred_element_type=jnp.float32)
        hidden = (jax.nn.silu(gate) * upward).astype(jnp.bfloat16)
        hidden_blocks = jnp.transpose(hidden.reshape(-1, N_TP, FF // N_TP), (1, 0, 2)).astype(jnp.float32)
        down_blocks = down_mat.reshape(N_TP, FF // N_TP, D).astype(jnp.float32)
        partial_sums = jnp.einsum('jsf,jfd->jsd', hidden_blocks, down_blocks)
        rounded = lax.optimization_barrier(partial_sums.astype(jnp.bfloat16))
        return lax.optimization_barrier(jnp.sum(rounded.astype(jnp.float32), axis=0)).astype(jnp.bfloat16)
    results = lax.map(expert_pass, (table, w_gate, w_up, w_down)).reshape(EXPERTS, N_EP, CAP, D)
    picked = results[flat_ids, source, position].reshape(ROWS, TOP, D).astype(jnp.float32)
    expert_out = jnp.einsum('rkd,rk->rd', picked, route_weights).astype(jnp.bfloat16)
    return (heads_out, expert_out)
```

```python
import functools

import jax
import jax.numpy as jnp
from jax import lax
from jax.experimental import pallas as pl
from jax.experimental.pallas import tpu as pltpu
from jax.sharding import PartitionSpec as P

MESH = pl.DeviceIdType.MESH
F32 = jnp.float32
BF16 = jnp.bfloat16
RIGHT, LEFT = 0, 1


def dot(a, b):
    return jnp.dot(a, b, preferred_element_type=F32)


def dot_nt(a, b):
    return lax.dot_general(a, b, (((1,), (1,)), ((), ())), preferred_element_type=F32)


def iota(shape, dim):
    return lax.broadcasted_iota(jnp.int32, shape, dim)


def kernel(
    E,
    T,
    q_hbm,
    k_hbm,
    v_hbm,
    lam_ref,
    hgain_hbm,
    tok_hbm,
    ids_hbm,
    rw_hbm,
    mgain_hbm,
    wg_hbm,
    wu_hbm,
    wd_hbm,
    heads_ref,
    eout_ref,
    q_s,
    hgain_s,
    tok_s,
    ids_s,
    rw_s,
    mgain_s,
    wg_s,
    wu_s,
    wd_s,
    normed_s,
    out_s,
    G,
    H,
    wts_a,
    wts_p,
    wts_q,
    dsend,
    drecv,
    res,
    back,
    Kb,
    Vb,
    scores,
    loc,
    b_send,
    b_recv,
    x_send,
    x_recv,
    d_send,
    d_recv,
    e_send,
    e_recv,
    kv_send,
    kv_recv,
    sib_send,
    sib_recv,
):
    ep, tp = lax.axis_index("ep"), lax.axis_index("tp")
    nb = E // T
    Z = E // 2
    rows, width = tok_s.shape
    cap = out_s.shape[0] // nb
    lanes = 128
    tail = cap // 2

    x_to = (lax.rem(tp + 1, T), lax.rem(tp + T - 1, T))
    z_to = (lax.rem(ep + 2, E), lax.rem(ep + E - 2, E))
    sibling = ep + 1 - 2 * lax.rem(ep, 2)
    own_high = ep // T

    def hops(b):
        return (T // 2, T // 2 - 1) if b % 2 == 0 else (T // 2 - 1, T // 2)

    near_first = sorted(range(nb), key=lambda b: (min(b, nb - b), b))
    far_first = near_first[::-1]

    barrier = pltpu.get_barrier_semaphore()

    def greet(i, _):
        pl.semaphore_signal(
            barrier, inc=1, device_id={"ep": lax.rem(ep + i, E)}, device_id_type=MESH
        )
        return 0

    lax.fori_loop(1, E, greet, 0)
    for to in x_to:
        pl.semaphore_signal(barrier, inc=1, device_id={"tp": to}, device_id_type=MESH)

    local = [
        pltpu.make_async_copy(src, dst, loc.at[i])
        for i, (src, dst) in enumerate(
            (
                (ids_hbm, ids_s),
                (tok_hbm, tok_s),
                (mgain_hbm, mgain_s),
                (k_hbm, Kb.at[ep]),
                (v_hbm, Vb.at[ep]),
                (wg_hbm, wg_s),
                (wu_hbm, wu_s),
                (rw_hbm, rw_s),
                (wd_hbm, wd_s),
                (q_hbm, q_s),
                (hgain_hbm, hgain_s),
            )
        )
    ]
    c_ids, c_tok, c_mgain, c_k, c_v, c_wg, c_wu, c_rw, c_wd, c_q, c_hgain = local
    for copy in local:
        copy.start()

    c_ids.wait()
    id0, id1 = ids_s[:, 0:1], ids_s[:, 1:2]
    lower = (iota((rows, rows), 1) < iota((rows, rows), 0)).astype(F32).astype(BF16)
    first = lax.rem(tp - lax.rem(ep, T) + T, T)
    lane = iota((rows, nb * cap), 1)
    lane_slot = lax.rem(lane, cap)
    lane_block = lane // cap
    lane_expert = first + T * lax.rem(own_high + nb - lane_block, nb)
    named = (id0 == lane_expert) | (id1 == lane_expert)
    earlier = dot(lower, named.astype(F32).astype(BF16))
    chosen = jnp.where(named & (earlier == lane_slot.astype(F32)), 1.0, 0.0)
    select = jnp.transpose(chosen).astype(BF16)

    c_tok.wait()
    c_mgain.wait()
    gain = mgain_s[...]
    step_rows = 32

    def norm(i, _):
        at = pl.ds(pl.multiple_of(i * step_rows, step_rows), step_rows)
        x = tok_s[at, :].astype(F32)
        scale = lax.rsqrt(jnp.mean(x * x, axis=1, keepdims=True) + 1e-06)
        normed_s[at, :] = (x * scale * gain).astype(BF16)
        return 0

    lax.fori_loop(0, rows // step_rows, norm, 0)
    out_s[...] = dot(select, normed_s[...]).astype(BF16)

    pl.semaphore_wait(barrier, E + 1)

    def block(b):
        return pl.ds(b * cap, cap)

    def expert_of(b):
        return first + T * lax.rem(own_high + nb - b, nb)

    def dispatch(b):
        return pltpu.make_async_remote_copy(
            src_ref=out_s.at[block(b)],
            dst_ref=G.at[tp, block(b)],
            send_sem=b_send.at[b],
            recv_sem=b_recv.at[b],
            device_id={"ep": expert_of(b)},
            device_id_type=MESH,
        )

    def dispatch_here(b):
        return pltpu.make_async_copy(out_s.at[block(b)], G.at[tp, block(b)], b_recv.at[b])

    for b in far_first:

        @pl.when(expert_of(b) != ep)
        def _():
            dispatch(b).start()

        @pl.when(expert_of(b) == ep)
        def _():
            dispatch_here(b).start()

    buffers = (Kb, Vb)
    kv_hops = ((Z // 2, Z // 2 - 1), (Z // 2 - 1, Z // 2))

    def kv_copy(which, way, step):
        origin = lax.rem(ep + (2 * step if way == LEFT else 2 * E - 2 * step), E)
        return pltpu.make_async_remote_copy(
            src_ref=buffers[which].at[origin],
            dst_ref=buffers[which].at[origin],
            send_sem=kv_send.at[which, way, step],
            recv_sem=kv_recv.at[which, way, step],
            device_id={"ep": z_to[way]},
            device_id_type=MESH,
        )

    def sib_copy(which, way, step):
        origin = lax.rem(ep + (2 * step if way == LEFT else 2 * E - 2 * step), E)
        return pltpu.make_async_remote_copy(
            src_ref=buffers[which].at[origin],
            dst_ref=buffers[which].at[origin],
            send_sem=sib_send.at[which],
            recv_sem=sib_recv.at[which],
            device_id={"ep": sibling},
            device_id_type=MESH,
        )

    c_k.wait()
    c_v.wait()
    for which in (0, 1):
        kv_copy(which, RIGHT, 0).start()
        kv_copy(which, LEFT, 0).start()
        sib_copy(which, RIGHT, 0).start()

    def kv_step(s):
        for which in (0, 1):
            for way in (RIGHT, LEFT):
                kv_copy(which, way, s - 1).wait_recv()
                kv_copy(which, way, s).start()
                sib_copy(which, way, s).start()

    def kv_step_before_last():
        s = Z // 2 - 1
        for which in (0, 1):
            for way in (RIGHT, LEFT):
                kv_copy(which, way, s - 1).wait_recv()
                if s < kv_hops[which][way]:
                    kv_copy(which, way, s).start()
                sib_copy(which, way, s).start()

    def kv_step_last():
        s = Z // 2
        for which, way in ((0, RIGHT), (1, LEFT)):
            kv_copy(which, way, s - 1).wait_recv()
            sib_copy(which, way, s).start()

    c_rw.wait()
    w0, w1 = rw_s[:, 0:1], rw_s[:, 1:2]
    lane_e = iota((rows, lanes), 1)
    hit0, hit1 = id0 == lane_e, id1 == lane_e
    before = dot(lower, jnp.where(hit0 | hit1, 1.0, 0.0).astype(BF16))
    pos0 = jnp.sum(jnp.where(hit0, before, 0.0), axis=1, keepdims=True)
    pos1 = jnp.sum(jnp.where(hit1, before, 0.0), axis=1, keepdims=True)
    f0, f1 = id0.astype(F32), id1.astype(F32)
    nowhere = -1.0

    def fill(ref, slot0, slot1):
        columns = ref.shape[2]

        def tile(i, _):
            at = pl.ds(pl.multiple_of(i * lanes, lanes), lanes)
            here = (iota((rows, lanes), 1) + i * lanes).astype(F32)
            w = jnp.where(here == slot0, w0, 0.0) + jnp.where(here == slot1, w1, 0.0)
            high = w.astype(BF16)
            ref[0, :, at] = high
            ref[1, :, at] = (w - high.astype(F32)).astype(BF16)
            return 0

        lax.fori_loop(0, columns // lanes, tile, 0)

    fill(wts_a, f0 * cap + pos0, f1 * cap + pos1)
    fill(
        wts_p,
        jnp.where(pos0 < tail, f0 * tail + pos0, nowhere),
        jnp.where(pos1 < tail, f1 * tail + pos1, nowhere),
    )
    fill(
        wts_q,
        jnp.where(pos0 >= tail, f0 * tail + pos0 - tail, nowhere),
        jnp.where(pos1 >= tail, f1 * tail + pos1 - tail, nowhere),
    )

    def ring_copy(b, way, step):
        origin = lax.rem(tp + (step if way == LEFT else T - step), T)
        return pltpu.make_async_remote_copy(
            src_ref=G.at[origin, block(b)],
            dst_ref=G.at[origin, block(b)],
            send_sem=x_send.at[way, b, step],
            recv_sem=x_recv.at[way, b, step],
            device_id={"tp": x_to[way]},
            device_id_type=MESH,
        )

    def hidden_of(origin):
        x = G[origin]
        gate = dot(x, wg_s[...])
        up = dot(x, wu_s[...])
        H[origin] = (gate / (1.0 + jnp.exp(-gate)) * up).astype(BF16)

    for b in near_first:
        dispatch_here(b).wait()
        for way in (RIGHT, LEFT):
            ring_copy(b, way, 0).start()

    c_wg.wait()
    c_wu.wait()
    hidden_of(tp)

    half = T // 2
    kv_per_step = Z // T

    def gather_step(s, _):
        for b in near_first:
            for way in (RIGHT, LEFT):
                ring_copy(b, way, s - 1).wait_recv()
                if hops(b)[way] == half:
                    ring_copy(b, way, s).start()
                else:

                    @pl.when(s < half - 1)
                    def _():
                        ring_copy(b, way, s).start()

        hidden_of(lax.rem(tp + T - s, T))
        for i in range(kv_per_step):
            kv_step(kv_per_step * (s - 1) + 1 + i)
        hidden_of(lax.rem(tp + s, T))
        return 0

    lax.fori_loop(1, half, gather_step, 0)
    for s in range(kv_per_step * (half - 1) + 1, Z // 2 - 1):
        kv_step(s)
    if Z // 2 > kv_per_step * (half - 1) + 1:
        kv_step_before_last()
    for b in near_first:
        for way in (RIGHT, LEFT):
            if hops(b)[way] == half:
                ring_copy(b, way, half - 1).wait_recv()
    hidden_of(lax.rem(tp + half, T))

    c_wd.wait()

    def own_part(target, b):
        pair, odd = target // 2, lax.rem(target, 2)
        h = H[:, block(b), :].reshape(T * cap, H.shape[2])
        wa = wd_s[:, pl.ds(pl.multiple_of((3 * pair + 2 * odd) * lanes, lanes), lanes)]
        wb = wd_s[:, pl.ds(pl.multiple_of((3 * pair + 1) * lanes, lanes), lanes)]
        a = dot(h, wa).reshape(T, cap, lanes)
        m = dot(h, wb)
        m = jnp.where(odd == 1, pltpu.roll(m, lanes // 2, 1), m)
        r = pltpu.roll(m, lanes // 2, 1).reshape(T, cap, lanes)[:, tail:]
        m = m.reshape(T, cap, lanes)[:, :tail]
        low = iota((T, tail, lanes), 2) < lanes // 2
        return a, jnp.where(low, m, r)

    def partial_copy(b, way, step):
        return pltpu.make_async_remote_copy(
            src_ref=dsend.at[way, b, step],
            dst_ref=drecv.at[way, b, step],
            send_sem=d_send.at[way, b, step],
            recv_sem=d_recv.at[way, b, step],
            device_id={"tp": x_to[way]},
            device_id_type=MESH,
        )

    def pass_on(b, way, step):
        left_to_go = hops(b)[way] - step
        target = lax.rem(tp + (left_to_go if way == RIGHT else T - left_to_go), T)
        a, m = own_part(target, b)
        if step > 0:
            partial_copy(b, way, step - 1).wait_recv()
            a = a + drecv[way, b, step - 1, :, :cap].astype(F32)
            m = m + drecv[way, b, step - 1, :, cap:].astype(F32)
        dsend[way, b, step, :, :cap] = a.astype(BF16)
        dsend[way, b, step, :, cap:] = m.astype(BF16)
        partial_copy(b, way, step).start()

    def source_of(b, j):
        return lax.rem(j + T - lax.rem(ep, T), T) + T * lax.rem(b + own_high, nb)

    def send_back(b, j):
        return pltpu.make_async_remote_copy(
            src_ref=res.at[b, j],
            dst_ref=back.at[ep],
            send_sem=e_send,
            recv_sem=e_recv,
            device_id={"ep": source_of(b, j)},
            device_id_type=MESH,
        )

    def finish(b):
        a, m = own_part(tp, b)
        for way in (RIGHT, LEFT):
            last = hops(b)[way] - 1
            partial_copy(b, way, last).wait_recv()
            a = a + drecv[way, b, last, :, :cap].astype(F32)
            m = m + drecv[way, b, last, :, cap:].astype(F32)
        res[b, :, :cap] = a.astype(BF16)
        res[b, :, cap:] = m.astype(BF16)

        def send(j, _):
            @pl.when(source_of(b, j) != ep)
            def _():
                send_back(b, j).start()

            @pl.when(source_of(b, j) == ep)
            def _():
                pltpu.make_async_copy(res.at[b, j], back.at[ep], e_recv).start()

            return 0

        lax.fori_loop(0, T, send, 0)

    def attend_scores(c):
        q = q_s[...]
        mine = (iota(q.shape, 1) >= lanes // 2) == (c == 1)
        scale = (lanes // 2) ** -0.5
        q = jnp.where(mine, q.astype(F32) * scale, 0.0).astype(BF16)
        group = 4
        keys = Kb.shape[1]

        def score(i, top):
            k = Kb[pl.ds(i * group, group)].reshape(group * keys, lanes)
            s = dot_nt(q, k)
            scores[:, pl.ds(pl.multiple_of(i * group * keys, group * keys), group * keys)] = s
            for g in range(group):
                top = jnp.maximum(top, s[:, g * keys : (g + 1) * keys])
            return top

        top = lax.fori_loop(0, E // group, score, jnp.full((q.shape[0], keys), -jnp.inf, F32))
        top = jnp.max(top, axis=1, keepdims=True)

        def weigh(i, carry):
            total, sums = carry
            at = pl.ds(pl.multiple_of(i * group * keys, group * keys), group * keys)
            w = jnp.exp(scores[:, at] - top)
            for g in range(group):
                total = total + w[:, g * keys : (g + 1) * keys]
            v = Vb[pl.ds(i * group, group)].reshape(group * keys, lanes)
            return total, sums + dot(w.astype(BF16), v)

        zero = jnp.zeros((q.shape[0], keys), F32)
        total, sums = lax.fori_loop(0, E // group, weigh, (zero, jnp.zeros(q.shape, F32)))
        return sums / jnp.sum(total, axis=1, keepdims=True)

    pair_count = 2
    size = nb // pair_count
    pairs = [far_first[i * size : (i + 1) * size] for i in range(pair_count)]
    lag = half // 2
    means = {}
    for slot in range(half + 1 + lag):
        for p, members in enumerate(pairs):
            step = slot - p * lag
            if step < 0 or step > half:
                continue
            for b in members:
                for way in (RIGHT, LEFT):
                    if step < hops(b)[way]:
                        pass_on(b, way, step)
                if step == half:
                    finish(b)
        if slot == 0:
            kv_step_last()
        if slot == lag - 1:
            for which in (0, 1):
                pltpu.make_async_copy(
                    buffers[which].at[pl.ds(0, Z)],
                    buffers[which].at[pl.ds(0, Z)],
                    sib_recv.at[which],
                ).wait()
            c_q.wait()
            c_hgain.wait()
            means[0] = attend_scores(0)
        if slot == lag:
            means[1] = attend_scores(1)
            mixed = means[0] - lam_ref[0] * means[1]
            scale = lax.rsqrt(jnp.mean(mixed * mixed, axis=1, keepdims=True) + 1e-06)
            heads_ref[...] = (mixed * scale * hgain_s[...]).astype(BF16)

    pltpu.make_async_copy(back, back, e_recv).wait()
    wide = back[:, :cap, :].reshape(E * cap, lanes)
    packed = back[:, cap:, :].reshape(E * tail, lanes)
    a = dot(wts_a[0], wide) + dot(wts_a[1], wide)
    m = dot(wts_p[0], packed) + dot(wts_p[1], packed)
    n = dot(wts_q[0], packed) + dot(wts_q[1], packed)
    m = m + pltpu.roll(n, lanes // 2, 1)
    turned = pltpu.roll(a, lanes // 2, 1)
    low = iota(a.shape, 1) < lanes // 2
    odd = lax.rem(tp, 2) == 1
    eout_ref[:, :lanes] = jnp.where(odd, jnp.where(low, m, turned), a).astype(BF16)
    rest = jnp.where(odd, turned, m).astype(BF16)
    eout_ref[:, lanes:] = rest[:, : lanes // 2]

    for b in range(nb):

        @pl.when(expert_of(b) != ep)
        def _():
            dispatch(b).wait_send()

        for way in (RIGHT, LEFT):
            for step in range(hops(b)[way]):
                ring_copy(b, way, step).wait_send()
                partial_copy(b, way, step).wait_send()
    for which in (0, 1):
        for way in (RIGHT, LEFT):
            for step in range(kv_hops[which][way]):
                kv_copy(which, way, step).wait_send()
        pltpu.make_async_copy(
            buffers[which].at[pl.ds(0, Z)], buffers[which].at[pl.ds(0, Z)], sib_send.at[which]
        ).wait()
    pltpu.make_async_copy(back.at[pl.ds(0, E - 1)], back.at[pl.ds(0, E - 1)], e_send).wait()


def on_device(
    queries,
    keys,
    values,
    lambdas,
    head_gain,
    tokens,
    route_ids,
    route_weights,
    moe_gain,
    w_gate,
    w_up,
    w_down,
):
    E, T = lax.axis_size("ep"), lax.axis_size("tp")
    nb, Z = E // T, E // 2
    rows, width = tokens.shape
    cap = 2 * rows * route_ids.shape[1] // E
    q_rows, lanes = queries.shape
    units = w_gate.shape[2]
    slice_width = width // T
    block_rows = cap * slice_width // lanes
    half = T // 2
    dma = pltpu.SemaphoreType.DMA
    anywhere = pl.BlockSpec(memory_space=pl.ANY)
    scratch = [
        pltpu.VMEM((q_rows, lanes), BF16),
        pltpu.VMEM((1, lanes), F32),
        pltpu.VMEM((rows, width), BF16),
        pltpu.VMEM(route_ids.shape, jnp.int32),
        pltpu.VMEM(route_weights.shape, F32),
        pltpu.VMEM((1, width), F32),
        pltpu.VMEM((width, units), BF16),
        pltpu.VMEM((width, units), BF16),
        pltpu.VMEM((units, width), BF16),
        pltpu.VMEM((rows, width), BF16),
        pltpu.VMEM((nb * cap, width), BF16),
        pltpu.VMEM((T, nb * cap, width), BF16),
        pltpu.VMEM((T, nb * cap, units), BF16),
        pltpu.VMEM((2, rows, E * cap), BF16),
        pltpu.VMEM((2, rows, E * cap // 2), BF16),
        pltpu.VMEM((2, rows, E * cap // 2), BF16),
        pltpu.VMEM((2, nb, half, T, block_rows, lanes), BF16),
        pltpu.VMEM((2, nb, half, T, block_rows, lanes), BF16),
        pltpu.VMEM((nb, T, block_rows, lanes), BF16),
        pltpu.VMEM((E, block_rows, lanes), BF16),
        pltpu.VMEM((E, q_rows, lanes), BF16),
        pltpu.VMEM((E, q_rows, lanes), BF16),
        pltpu.VMEM((q_rows, E * q_rows), F32),
        dma((11,)),
        dma((nb,)),
        dma((nb,)),
        dma((2, nb, half)),
        dma((2, nb, half)),
        dma((2, nb, half)),
        dma((2, nb, half)),
        dma,
        dma,
        dma((2, 2, Z // 2)),
        dma((2, 2, Z // 2)),
        dma((2,)),
        dma((2,)),
    ]
    return pl.pallas_call(
        functools.partial(kernel, E, T),
        out_shape=(
            jax.ShapeDtypeStruct((q_rows, lanes), BF16),
            jax.ShapeDtypeStruct((rows, slice_width), BF16),
        ),
        in_specs=[anywhere] * 3
        + [pl.BlockSpec(memory_space=pltpu.SMEM)]
        + [anywhere] * 8,
        out_specs=(pl.BlockSpec(memory_space=pltpu.VMEM),) * 2,
        scratch_shapes=scratch,
        compiler_params=pltpu.CompilerParams(
            collective_id=0, has_side_effects=True, vmem_limit_bytes=48 * 1024 * 1024
        ),
    )(
        queries,
        keys,
        values,
        lambdas,
        head_gain.reshape(1, -1),
        tokens,
        route_ids,
        route_weights,
        moe_gain.reshape(1, -1),
        w_gate.reshape(w_gate.shape[1:]),
        w_up.reshape(w_up.shape[1:]),
        w_down.reshape(w_down.shape[1:]),
    )


def solution(mesh):
    in_specs = (
        P(("grp", "ep"), "tp"),
        P(("grp", "ep"), "tp"),
        P(("grp", "ep"), "tp"),
        P("tp"),
        P(),
        P(("grp", "ep"), None),
        P(("grp", "ep"), None),
        P(("grp", "ep"), None),
        P(),
        P("ep", None, "tp"),
        P("ep", None, "tp"),
        P("ep", "tp", None),
    )
    out_specs = (P(("grp", "ep"), "tp"), P(("grp", "ep"), "tp"))
    return jax.shard_map(
        on_device, mesh=mesh, in_specs=in_specs, out_specs=out_specs, check_vma=False
    )
```

```python
import functools

import jax
import jax.numpy as jnp
from jax import lax
from jax.experimental import pallas as pl
from jax.experimental.pallas import tpu as pltpu
from jax.sharding import PartitionSpec as P

MESH = pl.DeviceIdType.MESH
F32 = jnp.float32
BF16 = jnp.bfloat16
RIGHT, LEFT = 0, 1


def dot(a, b):
    return jnp.dot(a, b, preferred_element_type=F32)


def dot_nt(a, b):
    return lax.dot_general(a, b, (((1,), (1,)), ((), ())), preferred_element_type=F32)


def iota(shape, dim):
    return lax.broadcasted_iota(jnp.int32, shape, dim)


def kernel(
    E,
    T,
    q_hbm,
    k_hbm,
    v_hbm,
    lam_ref,
    hgain_hbm,
    tok_hbm,
    ids_hbm,
    rw_hbm,
    mgain_hbm,
    wg_hbm,
    wu_hbm,
    wd_hbm,
    heads_ref,
    eout_ref,
    q_s,
    hgain_s,
    tok_s,
    ids_s,
    rw_s,
    mgain_s,
    wg_s,
    wu_s,
    wd_s,
    normed_s,
    out_s,
    G,
    H,
    wts_a,
    wts_p,
    wts_q,
    dsend,
    drecv,
    res,
    back,
    Kb,
    Vb,
    scores,
    loc,
    joined,
    b_send,
    b_recv,
    x_send,
    x_recv,
    d_send,
    d_recv,
    e_send,
    e_recv,
    kv_send,
    kv_recv,
    sib_send,
    sib_recv,
):
    ep, tp = lax.axis_index("ep"), lax.axis_index("tp")
    nb = E // T
    Z = E // 2
    rows, width = tok_s.shape
    cap = out_s.shape[1]
    lanes = 128
    tail = cap // 2
    level = ep // 2

    x_to = (lax.rem(tp + 1, T), lax.rem(tp + T - 1, T))
    z_to = (lax.rem(ep + 2, E), lax.rem(ep + E - 2, E))
    sibling = ep + 1 - 2 * lax.rem(ep, 2)
    own_high = ep // T

    def hops(b):
        return (T // 2, T // 2 - 1) if b % 2 == 0 else (T // 2 - 1, T // 2)

    near_first = sorted(range(nb), key=lambda b: (min(b, nb - b), b))
    far_first = near_first[::-1]

    barrier = pltpu.get_barrier_semaphore()

    def greet(i, _):
        @pl.when(i != ep)
        def _():
            pl.semaphore_signal(barrier, inc=1, device_id={"ep": i}, device_id_type=MESH)

        return 0

    lax.fori_loop(2 * level, E, greet, 0)
    for to in x_to:
        pl.semaphore_signal(barrier, inc=1, device_id={"tp": to}, device_id_type=MESH)

    local = [
        pltpu.make_async_copy(src, dst, loc.at[i])
        for i, (src, dst) in enumerate(
            (
                (ids_hbm, ids_s),
                (tok_hbm, tok_s),
                (mgain_hbm, mgain_s),
                (k_hbm, Kb.at[ep]),
                (v_hbm, Vb.at[ep]),
                (wg_hbm, wg_s),
                (wu_hbm, wu_s),
                (rw_hbm, rw_s),
                (wd_hbm, wd_s),
                (q_hbm, q_s),
                (hgain_hbm, hgain_s),
            )
        )
    ]
    c_ids, c_tok, c_mgain, c_k, c_v, c_wg, c_wu, c_rw, c_wd, c_q, c_hgain = local
    for copy in local:
        copy.start()

    pl.semaphore_wait(barrier, 2 * level + 3)

    def report(i, _):
        pl.semaphore_signal(joined.at[ep], inc=1, device_id={"ep": i}, device_id_type=MESH)
        return 0

    lax.fori_loop(0, 2 * level, report, 0)

    def column(row):
        return jnp.transpose(jnp.broadcast_to(row, (lanes, rows)))

    c_ids.wait()
    ids = ids_s[...].astype(F32)
    id0, id1 = column(ids[0:1]), column(ids[1:2])
    lower = (iota((rows, rows), 1) < iota((rows, rows), 0)).astype(F32).astype(BF16)
    first = lax.rem(tp - lax.rem(ep, T) + T, T)
    lane = iota((rows, nb * cap), 1)
    lane_slot = lax.rem(lane, cap).astype(F32)
    lane_expert = (first + T * (lane // cap)).astype(F32)
    named = (id0 == lane_expert) | (id1 == lane_expert)
    earlier = dot(lower, named.astype(F32).astype(BF16))
    chosen = jnp.where(named & (earlier == lane_slot), 1.0, 0.0)
    select = jnp.transpose(chosen).astype(BF16)

    c_tok.wait()
    c_mgain.wait()
    gain = mgain_s[...]
    step_rows = 32

    def norm(i, _):
        at = pl.ds(pl.multiple_of(i * step_rows, step_rows), step_rows)
        x = tok_s[at, :].astype(F32)
        scale = lax.rsqrt(jnp.mean(x * x, axis=1, keepdims=True) + 1e-06)
        normed_s[at, :] = (x * scale * gain).astype(BF16)
        return 0

    lax.fori_loop(0, rows // step_rows, norm, 0)
    out_s[...] = dot(select, normed_s[...]).astype(BF16).reshape(nb, cap, width)

    def dispatch(q):
        return pltpu.make_async_remote_copy(
            src_ref=out_s.at[q],
            dst_ref=G.at[own_high, tp],
            send_sem=b_send.at[q],
            recv_sem=b_recv.at[own_high],
            device_id={"ep": first + T * q},
            device_id_type=MESH,
        )

    def arrived(g):
        return pltpu.make_async_copy(G.at[g, tp], G.at[g, tp], b_recv.at[g])

    for q in range(nb):
        expert = first + T * q

        @pl.when((expert // 2 <= level) & (expert != ep))
        def _():
            dispatch(q).start()

        @pl.when(expert == ep)
        def _():
            pltpu.make_async_copy(out_s.at[q], G.at[own_high, tp], b_recv.at[own_high]).start()

    def later(z, _):
        pl.semaphore_wait(joined.at[2 * z], 1)
        pl.semaphore_wait(joined.at[2 * z + 1], 1)
        q = z // (T // 2)

        @pl.when((first + T * q) // 2 == z)
        def _():
            dispatch(q).start()

        return 0

    lax.fori_loop(level + 1, Z, later, 0)

    buffers = (Kb, Vb)
    kv_hops = ((Z // 2, Z // 2 - 1), (Z // 2 - 1, Z // 2))

    def kv_copy(which, way, step):
        origin = lax.rem(ep + (2 * step if way == LEFT else 2 * E - 2 * step), E)
        return pltpu.make_async_remote_copy(
            src_ref=buffers[which].at[origin],
            dst_ref=buffers[which].at[origin],
            send_sem=kv_send.at[which, way, step],
            recv_sem=kv_recv.at[which, way, step],
            device_id={"ep": z_to[way]},
            device_id_type=MESH,
        )

    def sib_copy(which, way, step):
        origin = lax.rem(ep + (2 * step if way == LEFT else 2 * E - 2 * step), E)
        return pltpu.make_async_remote_copy(
            src_ref=buffers[which].at[origin],
            dst_ref=buffers[which].at[origin],
            send_sem=sib_send.at[which],
            recv_sem=sib_recv.at[which],
            device_id={"ep": sibling},
            device_id_type=MESH,
        )

    c_k.wait()
    c_v.wait()
    for which in (0, 1):
        kv_copy(which, RIGHT, 0).start()
        kv_copy(which, LEFT, 0).start()
        sib_copy(which, RIGHT, 0).start()

    def kv_step(s):
        for which in (0, 1):
            for way in (RIGHT, LEFT):
                kv_copy(which, way, s - 1).wait_recv()
                kv_copy(which, way, s).start()
                sib_copy(which, way, s).start()

    def kv_step_before_last():
        s = Z // 2 - 1
        for which in (0, 1):
            for way in (RIGHT, LEFT):
                kv_copy(which, way, s - 1).wait_recv()
                if s < kv_hops[which][way]:
                    kv_copy(which, way, s).start()
                sib_copy(which, way, s).start()

    def kv_step_last():
        s = Z // 2
        for which, way in ((0, RIGHT), (1, LEFT)):
            kv_copy(which, way, s - 1).wait_recv()
            sib_copy(which, way, s).start()

    def ring_copy(g, way, step):
        origin = lax.rem(tp + (step if way == LEFT else T - step), T)
        return pltpu.make_async_remote_copy(
            src_ref=G.at[g, origin],
            dst_ref=G.at[g, origin],
            send_sem=x_send.at[way, g, step],
            recv_sem=x_recv.at[way, g, step],
            device_id={"tp": x_to[way]},
            device_id_type=MESH,
        )

    def hidden_of(origin):
        x = G[:, origin].reshape(nb * cap, width)
        gate = dot(x, wg_s[...])
        up = dot(x, wu_s[...])
        hidden = (gate / (1.0 + jnp.exp(-gate)) * up).astype(BF16)
        H[:, origin] = hidden.reshape(nb, cap, hidden.shape[1])

    for g in range(nb):
        arrived(g).wait()
        for way in (RIGHT, LEFT):
            ring_copy(g, way, 0).start()

    c_rw.wait()
    w0, w1 = column(rw_s[0:1, :]), column(rw_s[1:2, :])
    lane_e = iota((rows, lanes), 1).astype(F32)
    hit0, hit1 = id0 == lane_e, id1 == lane_e
    before = dot(lower, jnp.where(hit0 | hit1, 1.0, 0.0).astype(BF16))
    pos0 = jnp.sum(jnp.where(hit0, before, 0.0), axis=1, keepdims=True)
    pos1 = jnp.sum(jnp.where(hit1, before, 0.0), axis=1, keepdims=True)
    nowhere = -1.0

    def fill(ref, slot0, slot1):
        columns = ref.shape[2]

        def tile(i, _):
            at = pl.ds(pl.multiple_of(i * lanes, lanes), lanes)
            here = (iota((rows, lanes), 1) + i * lanes).astype(F32)
            w = jnp.where(here == slot0, w0, 0.0) + jnp.where(here == slot1, w1, 0.0)
            high = w.astype(BF16)
            ref[0, :, at] = high
            ref[1, :, at] = (w - high.astype(F32)).astype(BF16)
            return 0

        lax.fori_loop(0, columns // lanes, tile, 0)

    fill(wts_a, id0 * cap + pos0, id1 * cap + pos1)
    fill(
        wts_p,
        jnp.where(pos0 < tail, id0 * tail + pos0, nowhere),
        jnp.where(pos1 < tail, id1 * tail + pos1, nowhere),
    )
    fill(
        wts_q,
        jnp.where(pos0 >= tail, id0 * tail + pos0 - tail, nowhere),
        jnp.where(pos1 >= tail, id1 * tail + pos1 - tail, nowhere),
    )

    c_wg.wait()
    c_wu.wait()
    hidden_of(tp)

    half = T // 2
    kv_per_step = Z // T

    def gather_step(s, _):
        for b in range(nb):
            for way in (RIGHT, LEFT):
                ring_copy(b, way, s - 1).wait_recv()
                if hops(b)[way] == half:
                    ring_copy(b, way, s).start()
                else:

                    @pl.when(s < half - 1)
                    def _():
                        ring_copy(b, way, s).start()

        hidden_of(lax.rem(tp + T - s, T))
        for i in range(kv_per_step):
            kv_step(kv_per_step * (s - 1) + 1 + i)
        hidden_of(lax.rem(tp + s, T))
        return 0

    lax.fori_loop(1, half, gather_step, 0)
    for s in range(kv_per_step * (half - 1) + 1, Z // 2 - 1):
        kv_step(s)
    if Z // 2 > kv_per_step * (half - 1) + 1:
        kv_step_before_last()
    for b in range(nb):
        for way in (RIGHT, LEFT):
            if hops(b)[way] == half:
                ring_copy(b, way, half - 1).wait_recv()
    hidden_of(lax.rem(tp + half, T))

    c_wd.wait()

    def own_part(target, b):
        pair, odd = target // 2, lax.rem(target, 2)
        h = H[lax.rem(b + own_high, nb)].reshape(T * cap, H.shape[3])
        wa = wd_s[:, pl.ds(pl.multiple_of((3 * pair + 2 * odd) * lanes, lanes), lanes)]
        wb = wd_s[:, pl.ds(pl.multiple_of((3 * pair + 1) * lanes, lanes), lanes)]
        a = dot(h, wa).reshape(T, cap, lanes)
        m = dot(h, wb)
        m = jnp.where(odd == 1, pltpu.roll(m, lanes // 2, 1), m)
        r = pltpu.roll(m, lanes // 2, 1).reshape(T, cap, lanes)[:, tail:]
        m = m.reshape(T, cap, lanes)[:, :tail]
        low = iota((T, tail, lanes), 2) < lanes // 2
        return a, jnp.where(low, m, r)

    def partial_copy(b, way, step):
        return pltpu.make_async_remote_copy(
            src_ref=dsend.at[way, b, step],
            dst_ref=drecv.at[way, b, step],
            send_sem=d_send.at[way, b, step],
            recv_sem=d_recv.at[way, b, step],
            device_id={"tp": x_to[way]},
            device_id_type=MESH,
        )

    def pass_on(b, way, step):
        left_to_go = hops(b)[way] - step
        target = lax.rem(tp + (left_to_go if way == RIGHT else T - left_to_go), T)
        a, m = own_part(target, b)
        if step > 0:
            partial_copy(b, way, step - 1).wait_recv()
            a = a + drecv[way, b, step - 1, :, :cap].astype(F32)
            m = m + drecv[way, b, step - 1, :, cap:].astype(F32)
        dsend[way, b, step, :, :cap] = a.astype(BF16)
        dsend[way, b, step, :, cap:] = m.astype(BF16)
        partial_copy(b, way, step).start()

    def source_of(b, j):
        return lax.rem(j + T - lax.rem(ep, T), T) + T * lax.rem(b + own_high, nb)

    def send_back(b, j):
        return pltpu.make_async_remote_copy(
            src_ref=res.at[b, j],
            dst_ref=back.at[ep],
            send_sem=e_send,
            recv_sem=e_recv,
            device_id={"ep": source_of(b, j)},
            device_id_type=MESH,
        )

    def finish(b):
        a, m = own_part(tp, b)
        for way in (RIGHT, LEFT):
            last = hops(b)[way] - 1
            partial_copy(b, way, last).wait_recv()
            a = a + drecv[way, b, last, :, :cap].astype(F32)
            m = m + drecv[way, b, last, :, cap:].astype(F32)
        res[b, :, :cap] = a.astype(BF16)
        res[b, :, cap:] = m.astype(BF16)

        def send(j, _):
            @pl.when(source_of(b, j) != ep)
            def _():
                send_back(b, j).start()

            @pl.when(source_of(b, j) == ep)
            def _():
                pltpu.make_async_copy(res.at[b, j], back.at[ep], e_recv).start()

            return 0

        lax.fori_loop(0, T, send, 0)

    def attend_scores(c):
        q = q_s[...]
        mine = (iota(q.shape, 1) >= lanes // 2) == (c == 1)
        scale = (lanes // 2) ** -0.5
        q = jnp.where(mine, q.astype(F32) * scale, 0.0).astype(BF16)
        group = 4
        keys = Kb.shape[1]

        def score(i, top):
            k = Kb[pl.ds(i * group, group)].reshape(group * keys, lanes)
            s = dot_nt(q, k)
            scores[:, pl.ds(pl.multiple_of(i * group * keys, group * keys), group * keys)] = s
            for g in range(group):
                top = jnp.maximum(top, s[:, g * keys : (g + 1) * keys])
            return top

        top = lax.fori_loop(0, E // group, score, jnp.full((q.shape[0], keys), -jnp.inf, F32))
        top = jnp.max(top, axis=1, keepdims=True)

        def weigh(i, carry):
            total, sums = carry
            at = pl.ds(pl.multiple_of(i * group * keys, group * keys), group * keys)
            w = jnp.exp(scores[:, at] - top)
            for g in range(group):
                total = total + w[:, g * keys : (g + 1) * keys]
            v = Vb[pl.ds(i * group, group)].reshape(group * keys, lanes)
            return total, sums + dot(w.astype(BF16), v)

        zero = jnp.zeros((q.shape[0], keys), F32)
        total, sums = lax.fori_loop(0, E // group, weigh, (zero, jnp.zeros(q.shape, F32)))
        return sums / jnp.sum(total, axis=1, keepdims=True)

    pair_count = 2
    size = nb // pair_count
    pairs = [far_first[i * size : (i + 1) * size] for i in range(pair_count)]
    lag = half // 2
    means = {}
    for slot in range(half + 1 + lag):
        for p, members in enumerate(pairs):
            step = slot - p * lag
            if step < 0 or step > half:
                continue
            for b in members:
                for way in (RIGHT, LEFT):
                    if step < hops(b)[way]:
                        pass_on(b, way, step)
                if step == half:
                    finish(b)
        if slot == 0:
            kv_step_last()
        if slot == lag:
            for which in (0, 1):
                pltpu.make_async_copy(
                    buffers[which].at[pl.ds(0, Z)],
                    buffers[which].at[pl.ds(0, Z)],
                    sib_recv.at[which],
                ).wait()
            c_q.wait()
            c_hgain.wait()
            means[0] = attend_scores(0)
        if slot == lag + 1:
            means[1] = attend_scores(1)
            mixed = means[0] - lam_ref[0] * means[1]
            scale = lax.rsqrt(jnp.mean(mixed * mixed, axis=1, keepdims=True) + 1e-06)
            heads_ref[...] = (mixed * scale * hgain_s[...]).astype(BF16)

    pltpu.make_async_copy(back, back, e_recv).wait()
    wide = back[:, :cap, :].reshape(E * cap, lanes)
    packed = back[:, cap:, :].reshape(E * tail, lanes)
    a = dot(wts_a[0], wide) + dot(wts_a[1], wide)
    m = dot(wts_p[0], packed) + dot(wts_p[1], packed)
    n = dot(wts_q[0], packed) + dot(wts_q[1], packed)
    m = m + pltpu.roll(n, lanes // 2, 1)
    turned = pltpu.roll(a, lanes // 2, 1)
    low = iota(a.shape, 1) < lanes // 2
    odd = lax.rem(tp, 2) == 1
    eout_ref[:, :lanes] = jnp.where(odd, jnp.where(low, m, turned), a).astype(BF16)
    rest = jnp.where(odd, turned, m).astype(BF16)
    eout_ref[:, lanes:] = rest[:, : lanes // 2]

    for b in range(nb):

        @pl.when(first + T * b != ep)
        def _():
            dispatch(b).wait_send()

        for way in (RIGHT, LEFT):
            for step in range(hops(b)[way]):
                ring_copy(b, way, step).wait_send()
                partial_copy(b, way, step).wait_send()
    for which in (0, 1):
        for way in (RIGHT, LEFT):
            for step in range(kv_hops[which][way]):
                kv_copy(which, way, step).wait_send()
        pltpu.make_async_copy(
            buffers[which].at[pl.ds(0, Z)], buffers[which].at[pl.ds(0, Z)], sib_send.at[which]
        ).wait()
    pltpu.make_async_copy(back.at[pl.ds(0, E - 1)], back.at[pl.ds(0, E - 1)], e_send).wait()


def on_device(
    queries,
    keys,
    values,
    lambdas,
    head_gain,
    tokens,
    route_ids,
    route_weights,
    moe_gain,
    w_gate,
    w_up,
    w_down,
):
    E, T = lax.axis_size("ep"), lax.axis_size("tp")
    nb, Z = E // T, E // 2
    rows, width = tokens.shape
    cap = 2 * rows * route_ids.shape[1] // E
    q_rows, lanes = queries.shape
    units = w_gate.shape[2]
    slice_width = width // T
    block_rows = cap * slice_width // lanes
    half = T // 2
    dma = pltpu.SemaphoreType.DMA
    anywhere = pl.BlockSpec(memory_space=pltpu.HBM)
    scratch = [
        pltpu.VMEM((q_rows, lanes), BF16),
        pltpu.VMEM((1, lanes), F32),
        pltpu.VMEM((rows, width), BF16),
        pltpu.VMEM(route_ids.shape[::-1], jnp.int32),
        pltpu.VMEM(route_weights.shape[::-1], F32),
        pltpu.VMEM((1, width), F32),
        pltpu.VMEM((width, units), BF16),
        pltpu.VMEM((width, units), BF16),
        pltpu.VMEM((units, width), BF16),
        pltpu.VMEM((rows, width), BF16),
        pltpu.VMEM((nb, cap, width), BF16),
        pltpu.VMEM((nb, T, cap, width), BF16),
        pltpu.VMEM((nb, T, cap, units), BF16),
        pltpu.VMEM((2, rows, E * cap), BF16),
        pltpu.VMEM((2, rows, E * cap // 2), BF16),
        pltpu.VMEM((2, rows, E * cap // 2), BF16),
        pltpu.VMEM((2, nb, half, T, block_rows, lanes), BF16),
        pltpu.VMEM((2, nb, half, T, block_rows, lanes), BF16),
        pltpu.VMEM((nb, T, block_rows, lanes), BF16),
        pltpu.VMEM((E, block_rows, lanes), BF16),
        pltpu.VMEM((E, q_rows, lanes), BF16),
        pltpu.VMEM((E, q_rows, lanes), BF16),
        pltpu.VMEM((q_rows, E * q_rows), F32),
        dma((11,)),
        pltpu.SemaphoreType.REGULAR((E,)),
        dma((nb,)),
        dma((nb,)),
        dma((2, nb, half)),
        dma((2, nb, half)),
        dma((2, nb, half)),
        dma((2, nb, half)),
        dma,
        dma,
        dma((2, 2, Z // 2)),
        dma((2, 2, Z // 2)),
        dma((2,)),
        dma((2,)),
    ]
    return pl.pallas_call(
        functools.partial(kernel, E, T),
        out_shape=(
            jax.ShapeDtypeStruct((q_rows, lanes), BF16),
            jax.ShapeDtypeStruct((rows, slice_width), BF16),
        ),
        in_specs=[anywhere] * 3
        + [pl.BlockSpec(memory_space=pltpu.SMEM)]
        + [anywhere] * 8,
        out_specs=(pl.BlockSpec(memory_space=pltpu.VMEM),) * 2,
        scratch_shapes=scratch,
        compiler_params=pltpu.CompilerParams(
            collective_id=0, has_side_effects=True, vmem_limit_bytes=62 * 1024 * 1024
        ),
    )(
        queries,
        keys,
        values,
        lambdas,
        head_gain.reshape(1, -1),
        tokens,
        route_ids.T,
        route_weights.T,
        moe_gain.reshape(1, -1),
        w_gate.reshape(w_gate.shape[1:]),
        w_up.reshape(w_up.shape[1:]),
        w_down.reshape(w_down.shape[1:]),
    )


def solution(mesh):
    in_specs = (
        P(("grp", "ep"), "tp"),
        P(("grp", "ep"), "tp"),
        P(("grp", "ep"), "tp"),
        P("tp"),
        P(),
        P(("grp", "ep"), None),
        P(("grp", "ep"), None),
        P(("grp", "ep"), None),
        P(),
        P("ep", None, "tp"),
        P("ep", None, "tp"),
        P("ep", "tp", None),
    )
    out_specs = (P(("grp", "ep"), "tp"), P(("grp", "ep"), "tp"))
    return jax.shard_map(
        on_device, mesh=mesh, in_specs=in_specs, out_specs=out_specs, check_vma=False
    )
```

```python
import functools

import jax
import jax.numpy as jnp
from jax import lax
from jax.experimental import pallas as pl
from jax.experimental.pallas import tpu as pltpu
from jax.sharding import PartitionSpec as P

MESH = pl.DeviceIdType.MESH
F32 = jnp.float32
BF16 = jnp.bfloat16
RIGHT, LEFT = 0, 1


def dot(a, b):
    return jnp.dot(a, b, preferred_element_type=F32)


def dot_nt(a, b):
    return lax.dot_general(a, b, (((1,), (1,)), ((), ())), preferred_element_type=F32)


def iota(shape, dim):
    return lax.broadcasted_iota(jnp.int32, shape, dim)


def kernel(
    E,
    T,
    q_hbm,
    k_hbm,
    v_hbm,
    lam_ref,
    hgain_hbm,
    tok_hbm,
    ids_hbm,
    rw_hbm,
    mgain_hbm,
    wg_hbm,
    wu_hbm,
    wd_hbm,
    heads_ref,
    eout_ref,
    q_s,
    hgain_s,
    tok_s,
    ids_s,
    rw_s,
    mgain_s,
    wg_s,
    wu_s,
    wd_s,
    normed_s,
    out_s,
    G,
    H,
    wts_a,
    wts_p,
    wts_q,
    dsend,
    drecv,
    res,
    back,
    Kb,
    Vb,
    scores,
    loc,
    joined,
    b_send,
    b_recv,
    x_send,
    x_recv,
    d_send,
    d_recv,
    e_send,
    e_recv,
    kv_send,
    kv_recv,
    sib_send,
    sib_recv,
):
    ep, tp = lax.axis_index("ep"), lax.axis_index("tp")
    nb = E // T
    Z = E // 2
    rows, width = tok_s.shape
    cap = out_s.shape[1]
    lanes = 128
    tail = cap // 2
    level = ep // 2

    x_to = (lax.rem(tp + 1, T), lax.rem(tp + T - 1, T))
    z_to = (lax.rem(ep + 2, E), lax.rem(ep + E - 2, E))
    sibling = ep + 1 - 2 * lax.rem(ep, 2)
    own_high = ep // T

    def partner(high, b):
        upper, under = high // 2, lax.rem(high, 2)
        upper = 1 - upper if b // 2 else upper
        under = 1 - under if b % 2 else under
        return 2 * upper + under

    def hops(b):
        return (T // 2, T // 2 - 1) if b % 2 == 0 else (T // 2 - 1, T // 2)

    near_first = sorted(range(nb), key=lambda b: (min(b, nb - b), b))
    far_first = near_first[::-1]

    barrier = pltpu.get_barrier_semaphore()

    def greet(i, _):
        @pl.when(i != ep)
        def _():
            pl.semaphore_signal(barrier, inc=1, device_id={"ep": i}, device_id_type=MESH)

        return 0

    lax.fori_loop(2 * level, E, greet, 0)
    for to in x_to:
        pl.semaphore_signal(barrier, inc=1, device_id={"tp": to}, device_id_type=MESH)

    local = [
        pltpu.make_async_copy(src, dst, loc.at[i])
        for i, (src, dst) in enumerate(
            (
                (ids_hbm, ids_s),
                (tok_hbm, tok_s),
                (mgain_hbm, mgain_s),
                (k_hbm, Kb.at[ep]),
                (v_hbm, Vb.at[ep]),
                (wg_hbm, wg_s),
                (wu_hbm, wu_s),
                (rw_hbm, rw_s),
                (wd_hbm, wd_s),
                (q_hbm, q_s),
                (hgain_hbm, hgain_s),
            )
        )
    ]
    c_ids, c_tok, c_mgain, c_k, c_v, c_wg, c_wu, c_rw, c_wd, c_q, c_hgain = local
    for copy in local:
        copy.start()

    pl.semaphore_wait(barrier, 2 * level + 3)

    def report(i, _):
        pl.semaphore_signal(joined.at[ep], inc=1, device_id={"ep": i}, device_id_type=MESH)
        return 0

    lax.fori_loop(0, 2 * level, report, 0)

    def column(row):
        return jnp.transpose(jnp.broadcast_to(row, (lanes, rows)))

    c_ids.wait()
    ids = ids_s[...].astype(F32)
    id0, id1 = column(ids[0:1]), column(ids[1:2])
    lower = (iota((rows, rows), 1) < iota((rows, rows), 0)).astype(F32).astype(BF16)
    first = lax.rem(tp - lax.rem(ep, T) + T, T)
    lane = iota((rows, nb * cap), 1)
    lane_slot = lax.rem(lane, cap).astype(F32)
    lane_expert = (first + T * (lane // cap)).astype(F32)
    named = (id0 == lane_expert) | (id1 == lane_expert)
    earlier = dot(lower, named.astype(F32).astype(BF16))
    chosen = jnp.where(named & (earlier == lane_slot), 1.0, 0.0)
    select = jnp.transpose(chosen).astype(BF16)

    c_tok.wait()
    c_mgain.wait()
    gain = jnp.concatenate([mgain_s[i : i + 1] for i in range(width // lanes)], axis=1)
    step_rows = 32

    def norm(i, _):
        at = pl.ds(pl.multiple_of(i * step_rows, step_rows), step_rows)
        x = tok_s[at, :].astype(F32)
        scale = lax.rsqrt(jnp.mean(x * x, axis=1, keepdims=True) + 1e-06)
        normed_s[at, :] = (x * scale * gain).astype(BF16)
        return 0

    lax.fori_loop(0, rows // step_rows, norm, 0)
    out_s[...] = dot(select, normed_s[...]).astype(BF16).reshape(nb, cap, width)

    def dispatch(q):
        return pltpu.make_async_remote_copy(
            src_ref=out_s.at[q],
            dst_ref=G.at[own_high, tp],
            send_sem=b_send.at[q],
            recv_sem=b_recv.at[own_high],
            device_id={"ep": first + T * q},
            device_id_type=MESH,
        )

    def arrived(g):
        return pltpu.make_async_copy(G.at[g, tp], G.at[g, tp], b_recv.at[g])

    for q in range(nb):
        expert = first + T * q

        @pl.when((expert // 2 <= level) & (expert != ep))
        def _():
            dispatch(q).start()

        @pl.when(expert == ep)
        def _():
            pltpu.make_async_copy(out_s.at[q], G.at[own_high, tp], b_recv.at[own_high]).start()

    def later(z, _):
        pl.semaphore_wait(joined.at[2 * z], 1)
        pl.semaphore_wait(joined.at[2 * z + 1], 1)
        q = z // (T // 2)

        @pl.when((first + T * q) // 2 == z)
        def _():
            dispatch(q).start()

        return 0

    lax.fori_loop(level + 1, Z, later, 0)

    buffers = (Kb, Vb)
    kv_hops = ((Z // 2, Z // 2 - 1), (Z // 2 - 1, Z // 2))

    def kv_copy(which, way, step):
        origin = lax.rem(ep + (2 * step if way == LEFT else 2 * E - 2 * step), E)
        return pltpu.make_async_remote_copy(
            src_ref=buffers[which].at[origin],
            dst_ref=buffers[which].at[origin],
            send_sem=kv_send,
            recv_sem=kv_recv.at[which, way, step],
            device_id={"ep": z_to[way]},
            device_id_type=MESH,
        )

    def sib_copy(which, way, step):
        origin = lax.rem(ep + (2 * step if way == LEFT else 2 * E - 2 * step), E)
        return pltpu.make_async_remote_copy(
            src_ref=buffers[which].at[origin],
            dst_ref=buffers[which].at[origin],
            send_sem=sib_send.at[which],
            recv_sem=sib_recv.at[which],
            device_id={"ep": sibling},
            device_id_type=MESH,
        )

    c_k.wait()
    c_v.wait()
    for which in (0, 1):
        kv_copy(which, RIGHT, 0).start()
        kv_copy(which, LEFT, 0).start()
        sib_copy(which, RIGHT, 0).start()

    def kv_step(s):
        for which in (0, 1):
            for way in (RIGHT, LEFT):
                if s <= kv_hops[which][way]:
                    kv_copy(which, way, s - 1).wait_recv()
                    if s < kv_hops[which][way]:
                        kv_copy(which, way, s).start()
                    sib_copy(which, way, s).start()

    half = T // 2
    pair_count = 2
    size = nb // pair_count

    def group(k):
        return partner(own_high, k)

    def ring_copy(k, way, step):
        origin = lax.rem(tp + (step if way == LEFT else T - step), T)
        return pltpu.make_async_remote_copy(
            src_ref=G.at[group(k), origin],
            dst_ref=G.at[group(k), origin],
            send_sem=x_send,
            recv_sem=x_recv.at[way, k, step],
            device_id={"tp": x_to[way]},
            device_id_type=MESH,
        )

    def hidden_of(p, origins):
        places = [(group(k), o) for k in range(p * size, (p + 1) * size) for o in origins]
        x = jnp.concatenate([G[g, o] for g, o in places], axis=0)
        gate = dot(x, wg_s[...])
        up = dot(x, wu_s[...])
        hidden = (gate / (1.0 + jnp.exp(-gate)) * up).astype(BF16)
        for i, (g, o) in enumerate(places):
            H[g, o] = hidden[i * cap : (i + 1) * cap]

    def combine_weights():
        c_rw.wait()
        w0, w1 = column(rw_s[0:1, :]), column(rw_s[1:2, :])
        lane_e = iota((rows, lanes), 1).astype(F32)
        hit0, hit1 = id0 == lane_e, id1 == lane_e
        before = dot(lower, jnp.where(hit0 | hit1, 1.0, 0.0).astype(BF16))
        pos0 = jnp.sum(jnp.where(hit0, before, 0.0), axis=1, keepdims=True)
        pos1 = jnp.sum(jnp.where(hit1, before, 0.0), axis=1, keepdims=True)
        nowhere = -1.0

        def fill(ref, slot0, slot1):
            columns = ref.shape[2]

            def tile(i, _):
                at = pl.ds(pl.multiple_of(i * lanes, lanes), lanes)
                here = (iota((rows, lanes), 1) + i * lanes).astype(F32)
                w = jnp.where(here == slot0, w0, 0.0) + jnp.where(here == slot1, w1, 0.0)
                high = w.astype(BF16)
                ref[0, :, at] = high
                ref[1, :, at] = (w - high.astype(F32)).astype(BF16)
                return 0

            lax.fori_loop(0, columns // lanes, tile, 0)

        fill(wts_a, id0 * cap + pos0, id1 * cap + pos1)
        fill(
            wts_p,
            jnp.where(pos0 < tail, id0 * tail + pos0, nowhere),
            jnp.where(pos1 < tail, id1 * tail + pos1, nowhere),
        )
        fill(
            wts_q,
            jnp.where(pos0 >= tail, id0 * tail + pos0 - tail, nowhere),
            jnp.where(pos1 >= tail, id1 * tail + pos1 - tail, nowhere),
        )

    def own_part(target, b):
        pair, odd = target // 2, lax.rem(target, 2)
        h = H[partner(own_high, b)].reshape(T * cap, H.shape[3])
        wa = wd_s[:, pl.ds(pl.multiple_of((3 * pair + 2 * odd) * lanes, lanes), lanes)]
        wb = wd_s[:, pl.ds(pl.multiple_of((3 * pair + 1) * lanes, lanes), lanes)]
        a = dot(h, wa).reshape(T, cap, lanes)
        m = dot(h, wb)
        m = jnp.where(odd == 1, pltpu.roll(m, lanes // 2, 1), m)
        r = pltpu.roll(m, lanes // 2, 1).reshape(T, cap, lanes)[:, tail:]
        m = m.reshape(T, cap, lanes)[:, :tail]
        low = iota((T, tail, lanes), 2) < lanes // 2
        return a, jnp.where(low, m, r)

    def place(b, way, step):
        return b * (T - 1) + (hops(b)[RIGHT] if way == LEFT else 0) + step

    def partial_copy(b, way, step):
        return pltpu.make_async_remote_copy(
            src_ref=dsend.at[place(b, way, step)],
            dst_ref=drecv.at[way, b, step],
            send_sem=d_send,
            recv_sem=d_recv.at[way, b, step],
            device_id={"tp": x_to[way]},
            device_id_type=MESH,
        )

    def pass_on(b, way, step):
        left_to_go = hops(b)[way] - step
        target = lax.rem(tp + (left_to_go if way == RIGHT else T - left_to_go), T)
        a, m = own_part(target, b)
        if step > 0:
            partial_copy(b, way, step - 1).wait_recv()
            a = a + drecv[way, b, step - 1, :, :cap].astype(F32)
            m = m + drecv[way, b, step - 1, :, cap:].astype(F32)
        dsend[place(b, way, step), :, :cap] = a.astype(BF16)
        dsend[place(b, way, step), :, cap:] = m.astype(BF16)
        partial_copy(b, way, step).start()

    def source_of(b, j):
        return lax.rem(j + T - lax.rem(ep, T), T) + T * partner(own_high, b)

    def send_back(b, j):
        return pltpu.make_async_remote_copy(
            src_ref=res.at[b, j],
            dst_ref=back.at[ep],
            send_sem=e_send,
            recv_sem=e_recv.at[own_high],
            device_id={"ep": source_of(b, j)},
            device_id_type=MESH,
        )

    def finish(b):
        a, m = own_part(tp, b)
        for way in (RIGHT, LEFT):
            last = hops(b)[way] - 1
            partial_copy(b, way, last).wait_recv()
            a = a + drecv[way, b, last, :, :cap].astype(F32)
            m = m + drecv[way, b, last, :, cap:].astype(F32)
        res[b, :, :cap] = a.astype(BF16)
        res[b, :, cap:] = m.astype(BF16)

        def send(j, _):
            @pl.when(source_of(b, j) != ep)
            def _():
                send_back(b, j).start()

            @pl.when(source_of(b, j) == ep)
            def _():
                pltpu.make_async_copy(res.at[b, j], back.at[ep], e_recv.at[own_high]).start()

            return 0

        lax.fori_loop(0, T, send, 0)

    def attend_scores(c):
        q = q_s[...]
        mine = (iota(q.shape, 1) >= lanes // 2) == (c == 1)
        scale = (lanes // 2) ** -0.5
        q = jnp.where(mine, q.astype(F32) * scale, 0.0).astype(BF16)
        group = 4
        keys = Kb.shape[1]

        def score(i, top):
            k = Kb[pl.ds(i * group, group)].reshape(group * keys, lanes)
            s = dot_nt(q, k)
            scores[:, pl.ds(pl.multiple_of(i * group * keys, group * keys), group * keys)] = s
            for g in range(group):
                top = jnp.maximum(top, s[:, g * keys : (g + 1) * keys])
            return top

        top = lax.fori_loop(0, E // group, score, jnp.full((q.shape[0], keys), -jnp.inf, F32))
        top = jnp.max(top, axis=1, keepdims=True)

        def weigh(i, carry):
            total, sums = carry
            at = pl.ds(pl.multiple_of(i * group * keys, group * keys), group * keys)
            w = jnp.exp(scores[:, at] - top)
            for g in range(group):
                total = total + w[:, g * keys : (g + 1) * keys]
            v = Vb[pl.ds(i * group, group)].reshape(group * keys, lanes)
            return total, sums + dot(w.astype(BF16), v)

        zero = jnp.zeros((q.shape[0], keys), F32)
        total, sums = lax.fori_loop(0, E // group, weigh, (zero, jnp.zeros(q.shape, F32)))
        return sums / jnp.sum(total, axis=1, keepdims=True)

    kv_left = list(range(1, Z // 2 + 1))
    begin = {2: half + 1, 3: half + 1, 1: half, 0: half + 2}
    for slot in range(max(begin.values()) + half + 1):
        for p in range(pair_count):
            s = slot - p
            if s < 0 or s > half:
                continue
            for k in range(p * size, (p + 1) * size):
                if s == 0:
                    arrived(group(k)).wait()
                for way in (RIGHT, LEFT):
                    if 0 < s <= hops(k)[way]:
                        ring_copy(k, way, s - 1).wait_recv()
                    if s < hops(k)[way]:
                        ring_copy(k, way, s).start()
            if slot == 0:
                combine_weights()
                c_wg.wait()
                c_wu.wait()
            if s == 0 or s == half:
                hidden_of(p, [lax.rem(tp + s, T)])
            else:
                hidden_of(p, [lax.rem(tp + T - s, T), lax.rem(tp + s, T)])
        if slot == half:
            c_wd.wait()
        for b in begin:
            step = slot - begin[b]
            if step < 0 or step > half:
                continue
            for way in (RIGHT, LEFT):
                if step < hops(b)[way]:
                    pass_on(b, way, step)
            if step == half:
                finish(b)
        if slot > 0 and kv_left:
            kv_step(kv_left.pop(0))

    for which in (0, 1):
        pltpu.make_async_copy(
            buffers[which].at[pl.ds(0, Z)], buffers[which].at[pl.ds(0, Z)], sib_recv.at[which]
        ).wait()
    c_q.wait()
    c_hgain.wait()
    mean0 = attend_scores(0)
    mean1 = attend_scores(1)
    mixed = mean0 - lam_ref[0] * mean1
    scale = lax.rsqrt(jnp.mean(mixed * mixed, axis=1, keepdims=True) + 1e-06)
    heads_ref[...] = (mixed * scale * hgain_s[...]).astype(BF16)

    def quarter(b, carry):
        high = partner(own_high, b)
        part = back.at[pl.ds(high * T, T)]
        pltpu.make_async_copy(part, part, e_recv.at[high]).wait()
        wide = part[:, :cap, :].reshape(T * cap, lanes)
        packed = part[:, cap:, :].reshape(T * tail, lanes)
        at = pl.ds(pl.multiple_of(high * T * cap, lanes), T * cap)
        at_tail = pl.ds(pl.multiple_of(high * T * tail, lanes), T * tail)
        a, m, n = carry
        a = a + dot(wts_a[0, :, at], wide) + dot(wts_a[1, :, at], wide)
        m = m + dot(wts_p[0, :, at_tail], packed) + dot(wts_p[1, :, at_tail], packed)
        n = n + dot(wts_q[0, :, at_tail], packed) + dot(wts_q[1, :, at_tail], packed)
        return a, m, n

    carry = (jnp.zeros((rows, lanes), F32),) * 3
    for b in far_first:
        carry = quarter(b, carry)
    a, m, n = carry
    m = m + pltpu.roll(n, lanes // 2, 1)
    turned = pltpu.roll(a, lanes // 2, 1)
    low = iota(a.shape, 1) < lanes // 2
    odd = lax.rem(tp, 2) == 1
    eout_ref[:, :lanes] = jnp.where(odd, jnp.where(low, m, turned), a).astype(BF16)
    rest = jnp.where(odd, turned, m).astype(BF16)
    eout_ref[:, lanes:] = rest[:, : lanes // 2]

    for b in range(nb):

        @pl.when(first + T * b != ep)
        def _():
            dispatch(b).wait_send()

    pltpu.make_async_copy(dsend, dsend, x_send).wait()
    pltpu.make_async_copy(dsend, dsend, d_send).wait()
    pltpu.make_async_copy(Kb.at[pl.ds(0, E - 2)], Kb.at[pl.ds(0, E - 2)], kv_send).wait()
    for which in (0, 1):
        pltpu.make_async_copy(
            buffers[which].at[pl.ds(0, Z)], buffers[which].at[pl.ds(0, Z)], sib_send.at[which]
        ).wait()
    pltpu.make_async_copy(back.at[pl.ds(0, E - 1)], back.at[pl.ds(0, E - 1)], e_send).wait()


def on_device(
    queries,
    keys,
    values,
    lambdas,
    head_gain,
    tokens,
    route_ids,
    route_weights,
    moe_gain,
    w_gate,
    w_up,
    w_down,
):
    E, T = lax.axis_size("ep"), lax.axis_size("tp")
    nb, Z = E // T, E // 2
    rows, width = tokens.shape
    cap = 2 * rows * route_ids.shape[1] // E
    q_rows, lanes = queries.shape
    units = w_gate.shape[2]
    slice_width = width // T
    block_rows = cap * slice_width // lanes
    half = T // 2
    dma = pltpu.SemaphoreType.DMA
    anywhere = pl.BlockSpec(memory_space=pltpu.HBM)
    scratch = [
        pltpu.VMEM((q_rows, lanes), BF16),
        pltpu.VMEM((1, lanes), F32),
        pltpu.VMEM((rows, width), BF16),
        pltpu.VMEM(route_ids.shape[::-1], jnp.int32),
        pltpu.VMEM(route_weights.shape[::-1], F32),
        pltpu.VMEM((width // lanes, lanes), F32),
        pltpu.VMEM((width, units), BF16),
        pltpu.VMEM((width, units), BF16),
        pltpu.VMEM((units, width), BF16),
        pltpu.VMEM((rows, width), BF16),
        pltpu.VMEM((nb, cap, width), BF16),
        pltpu.VMEM((nb, T, cap, width), BF16),
        pltpu.VMEM((nb, T, cap, units), BF16),
        pltpu.VMEM((2, rows, E * cap), BF16),
        pltpu.VMEM((2, rows, E * cap // 2), BF16),
        pltpu.VMEM((2, rows, E * cap // 2), BF16),
        pltpu.VMEM((nb * (T - 1), T, block_rows, lanes), BF16),
        pltpu.VMEM((2, nb, half, T, block_rows, lanes), BF16),
        pltpu.VMEM((nb, T, block_rows, lanes), BF16),
        pltpu.VMEM((E, block_rows, lanes), BF16),
        pltpu.VMEM((E, q_rows, lanes), BF16),
        pltpu.VMEM((E, q_rows, lanes), BF16),
        pltpu.VMEM((q_rows, E * q_rows), F32),
        dma((11,)),
        pltpu.SemaphoreType.REGULAR((E,)),
        dma((nb,)),
        dma((nb,)),
        dma,
        dma((2, nb, half)),
        dma,
        dma((2, nb, half)),
        dma,
        dma((nb,)),
        dma,
        dma((2, 2, Z // 2)),
        dma((2,)),
        dma((2,)),
    ]
    return pl.pallas_call(
        functools.partial(kernel, E, T),
        out_shape=(
            jax.ShapeDtypeStruct((q_rows, lanes), BF16),
            jax.ShapeDtypeStruct((rows, slice_width), BF16),
        ),
        in_specs=[anywhere] * 3
        + [pl.BlockSpec(memory_space=pltpu.SMEM)]
        + [anywhere] * 8,
        out_specs=(pl.BlockSpec(memory_space=pltpu.VMEM),) * 2,
        scratch_shapes=scratch,
        compiler_params=pltpu.CompilerParams(
            collective_id=0, has_side_effects=True, vmem_limit_bytes=62 * 1024 * 1024
        ),
    )(
        queries,
        keys,
        values,
        lambdas,
        head_gain.reshape(1, -1),
        tokens,
        route_ids.T,
        route_weights.T,
        moe_gain.reshape(-1, lanes),
        w_gate.reshape(w_gate.shape[1:]),
        w_up.reshape(w_up.shape[1:]),
        w_down.reshape(w_down.shape[1:]),
    )


def solution(mesh):
    in_specs = (
        P(("grp", "ep"), "tp"),
        P(("grp", "ep"), "tp"),
        P(("grp", "ep"), "tp"),
        P("tp"),
        P(),
        P(("grp", "ep"), None),
        P(("grp", "ep"), None),
        P(("grp", "ep"), None),
        P(),
        P("ep", None, "tp"),
        P("ep", None, "tp"),
        P("ep", "tp", None),
    )
    out_specs = (P(("grp", "ep"), "tp"), P(("grp", "ep"), "tp"))
    return jax.shard_map(
        on_device, mesh=mesh, in_specs=in_specs, out_specs=out_specs, check_vma=False
    )
```

```python
import functools

import jax
import jax.numpy as jnp
from jax import lax
from jax.experimental import pallas as pl
from jax.experimental.pallas import tpu as pltpu
from jax.sharding import PartitionSpec as P

MESH = pl.DeviceIdType.MESH
F32 = jnp.float32
BF16 = jnp.bfloat16
RIGHT, LEFT = 0, 1


def dot(a, b):
    return jnp.dot(a, b, preferred_element_type=F32)


def dot_nt(a, b):
    return lax.dot_general(a, b, (((1,), (1,)), ((), ())), preferred_element_type=F32)


def iota(shape, dim):
    return lax.broadcasted_iota(jnp.int32, shape, dim)


def kernel(
    E,
    T,
    q_hbm,
    k_hbm,
    v_hbm,
    lam_ref,
    hgain_hbm,
    tok_hbm,
    ids_hbm,
    rw_hbm,
    mgain_hbm,
    wg_hbm,
    wu_hbm,
    wd_hbm,
    heads_ref,
    eout_ref,
    q_s,
    hgain_s,
    tok_s,
    ids_s,
    rw_s,
    mgain_s,
    wg_s,
    wu_s,
    wd_s,
    normed_s,
    out_s,
    G,
    H,
    wts_a,
    wts_p,
    wts_q,
    dsend,
    drecv,
    res,
    back,
    Kb,
    Vb,
    scores,
    loc,
    joined,
    b_send,
    b_recv,
    x_send,
    x_recv,
    d_send,
    d_recv,
    e_send,
    e_recv,
    kv_send,
    kv_recv,
    sib_send,
    sib_recv,
):
    ep, tp = lax.axis_index("ep"), lax.axis_index("tp")
    nb = E // T
    Z = E // 2
    rows, width = tok_s.shape
    cap = out_s.shape[1]
    lanes = 128
    tail = cap // 2
    level = ep // 2

    x_to = (lax.rem(tp + 1, T), lax.rem(tp + T - 1, T))
    z_to = (lax.rem(ep + 2, E), lax.rem(ep + E - 2, E))
    sibling = ep + 1 - 2 * lax.rem(ep, 2)
    own_high = ep // T

    def partner(high, b):
        upper, under = high // 2, lax.rem(high, 2)
        upper = 1 - upper if b // 2 else upper
        under = 1 - under if b % 2 else under
        return 2 * upper + under

    def hops(b):
        return (T // 2, T // 2 - 1) if b % 2 == 0 else (T // 2 - 1, T // 2)

    near_first = sorted(range(nb), key=lambda b: (min(b, nb - b), b))
    far_first = near_first[::-1]

    barrier = pltpu.get_barrier_semaphore()

    def greet(i, _):
        @pl.when(i != ep)
        def _():
            pl.semaphore_signal(barrier, inc=1, device_id={"ep": i}, device_id_type=MESH)

        return 0

    lax.fori_loop(2 * level, E, greet, 0)
    for to in x_to:
        pl.semaphore_signal(barrier, inc=1, device_id={"tp": to}, device_id_type=MESH)

    local = [
        pltpu.make_async_copy(src, dst, loc.at[i])
        for i, (src, dst) in enumerate(
            (
                (ids_hbm, ids_s),
                (tok_hbm, tok_s),
                (mgain_hbm, mgain_s),
                (k_hbm, Kb.at[ep]),
                (v_hbm, Vb.at[ep]),
                (wg_hbm, wg_s),
                (wu_hbm, wu_s),
                (rw_hbm, rw_s),
                (wd_hbm, wd_s),
                (q_hbm, q_s),
                (hgain_hbm, hgain_s),
            )
        )
    ]
    c_ids, c_tok, c_mgain, c_k, c_v, c_wg, c_wu, c_rw, c_wd, c_q, c_hgain = local
    for copy in local:
        copy.start()

    pl.semaphore_wait(barrier, 2 * level + 3)

    def report(i, _):
        pl.semaphore_signal(joined.at[ep], inc=1, device_id={"ep": i}, device_id_type=MESH)
        return 0

    lax.fori_loop(0, 2 * level, report, 0)

    def column(row):
        return jnp.transpose(jnp.broadcast_to(row, (lanes, rows)))

    c_ids.wait()
    ids = ids_s[...].astype(F32)
    id0, id1 = column(ids[0:1]), column(ids[1:2])
    lower = (iota((rows, rows), 1) < iota((rows, rows), 0)).astype(F32).astype(BF16)
    first = lax.rem(tp - lax.rem(ep, T) + T, T)
    lane = iota((rows, nb * cap), 1)
    lane_slot = lax.rem(lane, cap).astype(F32)
    lane_expert = (first + T * (lane // cap)).astype(F32)
    named = (id0 == lane_expert) | (id1 == lane_expert)
    earlier = dot(lower, named.astype(F32).astype(BF16))
    chosen = jnp.where(named & (earlier == lane_slot), 1.0, 0.0)
    select = jnp.transpose(chosen).astype(BF16)

    c_tok.wait()
    c_mgain.wait()
    gain = jnp.concatenate([mgain_s[i : i + 1] for i in range(width // lanes)], axis=1)
    step_rows = 32

    def norm(i, _):
        at = pl.ds(pl.multiple_of(i * step_rows, step_rows), step_rows)
        x = tok_s[at, :].astype(F32)
        scale = lax.rsqrt(jnp.mean(x * x, axis=1, keepdims=True) + 1e-06)
        normed_s[at, :] = (x * scale * gain).astype(BF16)
        return 0

    lax.fori_loop(0, rows // step_rows, norm, 0)
    out_s[...] = dot(select, normed_s[...]).astype(BF16).reshape(nb, cap, width)

    def dispatch(q):
        return pltpu.make_async_remote_copy(
            src_ref=out_s.at[q],
            dst_ref=G.at[own_high, tp],
            send_sem=b_send.at[q],
            recv_sem=b_recv.at[own_high],
            device_id={"ep": first + T * q},
            device_id_type=MESH,
        )

    def arrived(g):
        return pltpu.make_async_copy(G.at[g, tp], G.at[g, tp], b_recv.at[g])

    for k in range(nb):
        q = partner(own_high, k)
        expert = first + T * q

        @pl.when((expert // 2 <= level) & (expert != ep))
        def _():
            dispatch(q).start()

        @pl.when(expert == ep)
        def _():
            pltpu.make_async_copy(out_s.at[q], G.at[own_high, tp], b_recv.at[own_high]).start()

    def later(z, _):
        pl.semaphore_wait(joined.at[2 * z], 1)
        pl.semaphore_wait(joined.at[2 * z + 1], 1)
        q = z // (T // 2)

        @pl.when((first + T * q) // 2 == z)
        def _():
            dispatch(q).start()

        return 0

    lax.fori_loop(level + 1, Z, later, 0)

    buffers = (Kb, Vb)
    kv_hops = ((Z // 2, Z // 2 - 1), (Z // 2 - 1, Z // 2))

    def kv_copy(which, way, step):
        origin = lax.rem(ep + (2 * step if way == LEFT else 2 * E - 2 * step), E)
        return pltpu.make_async_remote_copy(
            src_ref=buffers[which].at[origin],
            dst_ref=buffers[which].at[origin],
            send_sem=kv_send,
            recv_sem=kv_recv.at[which, way, step],
            device_id={"ep": z_to[way]},
            device_id_type=MESH,
        )

    def sib_copy(which, way, step):
        origin = lax.rem(ep + (2 * step if way == LEFT else 2 * E - 2 * step), E)
        return pltpu.make_async_remote_copy(
            src_ref=buffers[which].at[origin],
            dst_ref=buffers[which].at[origin],
            send_sem=sib_send.at[which],
            recv_sem=sib_recv.at[which],
            device_id={"ep": sibling},
            device_id_type=MESH,
        )

    c_k.wait()
    c_v.wait()
    for which in (0, 1):
        kv_copy(which, RIGHT, 0).start()
        kv_copy(which, LEFT, 0).start()
        sib_copy(which, RIGHT, 0).start()

    def kv_step(s):
        for which in (0, 1):
            for way in (RIGHT, LEFT):
                if s <= kv_hops[which][way]:
                    kv_copy(which, way, s - 1).wait_recv()
                    if s < kv_hops[which][way]:
                        kv_copy(which, way, s).start()
                    sib_copy(which, way, s).start()

    half = T // 2
    pair_count = 2
    size = nb // pair_count

    def group(k):
        return partner(own_high, k)

    def ring_copy(k, way, step):
        origin = lax.rem(tp + (step if way == LEFT else T - step), T)
        return pltpu.make_async_remote_copy(
            src_ref=G.at[group(k), origin],
            dst_ref=G.at[group(k), origin],
            send_sem=x_send,
            recv_sem=x_recv.at[way, k, step],
            device_id={"tp": x_to[way]},
            device_id_type=MESH,
        )

    def hidden_of(p, origins):
        places = [(group(k), o) for k in range(p * size, (p + 1) * size) for o in origins]
        x = jnp.concatenate([G[g, o] for g, o in places], axis=0)
        gate = dot(x, wg_s[...])
        up = dot(x, wu_s[...])
        hidden = (gate / (1.0 + jnp.exp(-gate)) * up).astype(BF16)
        for i, (g, o) in enumerate(places):
            H[g, o] = hidden[i * cap : (i + 1) * cap]

    def combine_weights():
        c_rw.wait()
        w0, w1 = column(rw_s[0:1, :]), column(rw_s[1:2, :])
        lane_e = iota((rows, lanes), 1).astype(F32)
        hit0, hit1 = id0 == lane_e, id1 == lane_e
        before = dot(lower, jnp.where(hit0 | hit1, 1.0, 0.0).astype(BF16))
        pos0 = jnp.sum(jnp.where(hit0, before, 0.0), axis=1, keepdims=True)
        pos1 = jnp.sum(jnp.where(hit1, before, 0.0), axis=1, keepdims=True)
        nowhere = -1.0

        def fill(ref, slot0, slot1):
            columns = ref.shape[2]

            def tile(i, _):
                at = pl.ds(pl.multiple_of(i * lanes, lanes), lanes)
                here = (iota((rows, lanes), 1) + i * lanes).astype(F32)
                w = jnp.where(here == slot0, w0, 0.0) + jnp.where(here == slot1, w1, 0.0)
                high = w.astype(BF16)
                ref[0, :, at] = high
                ref[1, :, at] = (w - high.astype(F32)).astype(BF16)
                return 0

            lax.fori_loop(0, columns // lanes, tile, 0)

        fill(wts_a, id0 * cap + pos0, id1 * cap + pos1)
        fill(
            wts_p,
            jnp.where(pos0 < tail, id0 * tail + pos0, nowhere),
            jnp.where(pos1 < tail, id1 * tail + pos1, nowhere),
        )
        fill(
            wts_q,
            jnp.where(pos0 >= tail, id0 * tail + pos0 - tail, nowhere),
            jnp.where(pos1 >= tail, id1 * tail + pos1 - tail, nowhere),
        )

    def own_part(target, b):
        pair, odd = target // 2, lax.rem(target, 2)
        h = H[partner(own_high, b)].reshape(T * cap, H.shape[3])
        wa = wd_s[:, pl.ds(pl.multiple_of((3 * pair + 2 * odd) * lanes, lanes), lanes)]
        wb = wd_s[:, pl.ds(pl.multiple_of((3 * pair + 1) * lanes, lanes), lanes)]
        a = dot(h, wa).reshape(T, cap, lanes)
        m = dot(h, wb)
        m = jnp.where(odd == 1, pltpu.roll(m, lanes // 2, 1), m)
        r = pltpu.roll(m, lanes // 2, 1).reshape(T, cap, lanes)[:, tail:]
        m = m.reshape(T, cap, lanes)[:, :tail]
        low = iota((T, tail, lanes), 2) < lanes // 2
        return a, jnp.where(low, m, r)

    def place(b, way, step):
        return b * (T - 1) + (hops(b)[RIGHT] if way == LEFT else 0) + step

    def partial_copy(b, way, step):
        return pltpu.make_async_remote_copy(
            src_ref=dsend.at[place(b, way, step)],
            dst_ref=drecv.at[way, b, step],
            send_sem=d_send,
            recv_sem=d_recv.at[way, b, step],
            device_id={"tp": x_to[way]},
            device_id_type=MESH,
        )

    def pass_on(b, way, step):
        left_to_go = hops(b)[way] - step
        target = lax.rem(tp + (left_to_go if way == RIGHT else T - left_to_go), T)
        a, m = own_part(target, b)
        if step > 0:
            partial_copy(b, way, step - 1).wait_recv()
            a = a + drecv[way, b, step - 1, :, :cap].astype(F32)
            m = m + drecv[way, b, step - 1, :, cap:].astype(F32)
        dsend[place(b, way, step), :, :cap] = a.astype(BF16)
        dsend[place(b, way, step), :, cap:] = m.astype(BF16)
        partial_copy(b, way, step).start()

    def source_of(b, j):
        return lax.rem(j + T - lax.rem(ep, T), T) + T * partner(own_high, b)

    def send_back(b, j):
        return pltpu.make_async_remote_copy(
            src_ref=res.at[b, j],
            dst_ref=back.at[ep],
            send_sem=e_send,
            recv_sem=e_recv.at[own_high],
            device_id={"ep": source_of(b, j)},
            device_id_type=MESH,
        )

    def finish(b):
        a, m = own_part(tp, b)
        for way in (RIGHT, LEFT):
            last = hops(b)[way] - 1
            partial_copy(b, way, last).wait_recv()
            a = a + drecv[way, b, last, :, :cap].astype(F32)
            m = m + drecv[way, b, last, :, cap:].astype(F32)
        res[b, :, :cap] = a.astype(BF16)
        res[b, :, cap:] = m.astype(BF16)

        def send(j, _):
            @pl.when(source_of(b, j) != ep)
            def _():
                send_back(b, j).start()

            @pl.when(source_of(b, j) == ep)
            def _():
                pltpu.make_async_copy(res.at[b, j], back.at[ep], e_recv.at[own_high]).start()

            return 0

        lax.fori_loop(0, T, send, 0)

    keys = Kb.shape[1]
    span = 4

    def attend():
        q = q_s[...].astype(F32) * (lanes // 2) ** -0.5
        first_half = iota(q.shape, 1) < lanes // 2
        q = jnp.concatenate([jnp.where(first_half, q, 0.0), jnp.where(first_half, 0.0, q)], axis=0)
        q = q.astype(BF16)
        top = jnp.full((2 * keys, keys), -jnp.inf, F32)
        for i in range(E // span):
            k = Kb[i * span : (i + 1) * span].reshape(span * keys, lanes)
            s = dot_nt(q, k)
            scores[:, i * span * keys : (i + 1) * span * keys] = s
            for g in range(span):
                top = jnp.maximum(top, s[:, g * keys : (g + 1) * keys])
        top = jnp.max(top, axis=1, keepdims=True)
        means = []
        for c in range(2):
            at_rows = slice(c * keys, (c + 1) * keys)
            high = jnp.broadcast_to(top[at_rows], (keys, span * keys))
            total = jnp.zeros((keys, keys), F32)
            sums = jnp.zeros((keys, lanes), F32)
            for i in range(E // span):
                w = jnp.exp(scores[at_rows, i * span * keys : (i + 1) * span * keys] - high)
                for g in range(span):
                    total = total + w[:, g * keys : (g + 1) * keys]
                v = Vb[i * span : (i + 1) * span].reshape(span * keys, lanes)
                sums = sums + dot(w.astype(BF16), v)
            means.append(sums / jnp.sum(total, axis=1, keepdims=True))
        return means

    kv_left = list(range(1, Z // 2 + 1))
    begin = {2: half + 1, 3: half + 1, 1: half, 0: half + 3}
    for slot in range(max(begin.values()) + half + 1):
        for p in range(pair_count):
            s = slot - p
            if s < 0 or s > half:
                continue
            for k in range(p * size, (p + 1) * size):
                if s == 0:
                    arrived(group(k)).wait()
                for way in (RIGHT, LEFT):
                    if 0 < s <= hops(k)[way]:
                        ring_copy(k, way, s - 1).wait_recv()
                    if s < hops(k)[way]:
                        ring_copy(k, way, s).start()
            if slot == 0:
                combine_weights()
                c_wg.wait()
                c_wu.wait()
            if s == 0 or s == half:
                hidden_of(p, [lax.rem(tp + s, T)])
            else:
                hidden_of(p, [lax.rem(tp + T - s, T), lax.rem(tp + s, T)])
        if slot == half:
            c_wd.wait()
        for b in begin:
            step = slot - begin[b]
            if step < 0 or step > half:
                continue
            for way in (RIGHT, LEFT):
                if step < hops(b)[way]:
                    pass_on(b, way, step)
            if step == half:
                finish(b)
        if slot > 0 and kv_left:
            kv_step(kv_left.pop(0))

    for which in (0, 1):
        pltpu.make_async_copy(
            buffers[which].at[pl.ds(0, Z)], buffers[which].at[pl.ds(0, Z)], sib_recv.at[which]
        ).wait()
    c_q.wait()
    c_hgain.wait()
    mean0, mean1 = attend()
    mixed = mean0 - lam_ref[0] * mean1
    scale = lax.rsqrt(jnp.mean(mixed * mixed, axis=1, keepdims=True) + 1e-06)
    heads_ref[...] = (mixed * scale * hgain_s[...]).astype(BF16)

    def quarter(b, carry):
        high = partner(own_high, b)
        part = back.at[pl.ds(high * T, T)]
        pltpu.make_async_copy(part, part, e_recv.at[high]).wait()
        wide = part[:, :cap, :].reshape(T * cap, lanes)
        packed = part[:, cap:, :].reshape(T * tail, lanes)
        at = pl.ds(pl.multiple_of(high * T * cap, lanes), T * cap)
        at_tail = pl.ds(pl.multiple_of(high * T * tail, lanes), T * tail)
        a, m, n = carry
        a = a + dot(wts_a[0, :, at], wide) + dot(wts_a[1, :, at], wide)
        m = m + dot(wts_p[0, :, at_tail], packed) + dot(wts_p[1, :, at_tail], packed)
        n = n + dot(wts_q[0, :, at_tail], packed) + dot(wts_q[1, :, at_tail], packed)
        return a, m, n

    carry = (jnp.zeros((rows, lanes), F32),) * 3
    for b in far_first:
        carry = quarter(b, carry)
    a, m, n = carry
    m = m + pltpu.roll(n, lanes // 2, 1)
    turned = pltpu.roll(a, lanes // 2, 1)
    low = iota(a.shape, 1) < lanes // 2
    odd = lax.rem(tp, 2) == 1
    eout_ref[:, :lanes] = jnp.where(odd, jnp.where(low, m, turned), a).astype(BF16)
    rest = jnp.where(odd, turned, m).astype(BF16)
    eout_ref[:, lanes:] = rest[:, : lanes // 2]

    for b in range(nb):

        @pl.when(first + T * b != ep)
        def _():
            dispatch(b).wait_send()

    pltpu.make_async_copy(dsend, dsend, x_send).wait()
    pltpu.make_async_copy(dsend, dsend, d_send).wait()
    pltpu.make_async_copy(Kb.at[pl.ds(0, E - 2)], Kb.at[pl.ds(0, E - 2)], kv_send).wait()
    for which in (0, 1):
        pltpu.make_async_copy(
            buffers[which].at[pl.ds(0, Z)], buffers[which].at[pl.ds(0, Z)], sib_send.at[which]
        ).wait()
    pltpu.make_async_copy(back.at[pl.ds(0, E - 1)], back.at[pl.ds(0, E - 1)], e_send).wait()


def on_device(
    queries,
    keys,
    values,
    lambdas,
    head_gain,
    tokens,
    route_ids,
    route_weights,
    moe_gain,
    w_gate,
    w_up,
    w_down,
):
    E, T = lax.axis_size("ep"), lax.axis_size("tp")
    nb, Z = E // T, E // 2
    rows, width = tokens.shape
    cap = 2 * rows * route_ids.shape[1] // E
    q_rows, lanes = queries.shape
    units = w_gate.shape[2]
    slice_width = width // T
    block_rows = cap * slice_width // lanes
    half = T // 2
    dma = pltpu.SemaphoreType.DMA
    anywhere = pl.BlockSpec(memory_space=pltpu.HBM)
    scratch = [
        pltpu.VMEM((q_rows, lanes), BF16),
        pltpu.VMEM((1, lanes), F32),
        pltpu.VMEM((rows, width), BF16),
        pltpu.VMEM(route_ids.shape[::-1], jnp.int32),
        pltpu.VMEM(route_weights.shape[::-1], F32),
        pltpu.VMEM((width // lanes, lanes), F32),
        pltpu.VMEM((width, units), BF16),
        pltpu.VMEM((width, units), BF16),
        pltpu.VMEM((units, width), BF16),
        pltpu.VMEM((rows, width), BF16),
        pltpu.VMEM((nb, cap, width), BF16),
        pltpu.VMEM((nb, T, cap, width), BF16),
        pltpu.VMEM((nb, T, cap, units), BF16),
        pltpu.VMEM((2, rows, E * cap), BF16),
        pltpu.VMEM((2, rows, E * cap // 2), BF16),
        pltpu.VMEM((2, rows, E * cap // 2), BF16),
        pltpu.VMEM((nb * (T - 1), T, block_rows, lanes), BF16),
        pltpu.VMEM((2, nb, half, T, block_rows, lanes), BF16),
        pltpu.VMEM((nb, T, block_rows, lanes), BF16),
        pltpu.VMEM((E, block_rows, lanes), BF16),
        pltpu.VMEM((E, q_rows, lanes), BF16),
        pltpu.VMEM((E, q_rows, lanes), BF16),
        pltpu.VMEM((2 * q_rows, E * q_rows), F32),
        dma((11,)),
        pltpu.SemaphoreType.REGULAR((E,)),
        dma((nb,)),
        dma((nb,)),
        dma,
        dma((2, nb, half)),
        dma,
        dma((2, nb, half)),
        dma,
        dma((nb,)),
        dma,
        dma((2, 2, Z // 2)),
        dma((2,)),
        dma((2,)),
    ]
    return pl.pallas_call(
        functools.partial(kernel, E, T),
        out_shape=(
            jax.ShapeDtypeStruct((q_rows, lanes), BF16),
            jax.ShapeDtypeStruct((rows, slice_width), BF16),
        ),
        in_specs=[anywhere] * 3
        + [pl.BlockSpec(memory_space=pltpu.SMEM)]
        + [anywhere] * 8,
        out_specs=(pl.BlockSpec(memory_space=pltpu.VMEM),) * 2,
        scratch_shapes=scratch,
        compiler_params=pltpu.CompilerParams(
            collective_id=0, has_side_effects=True, vmem_limit_bytes=62 * 1024 * 1024
        ),
    )(
        queries,
        keys,
        values,
        lambdas,
        head_gain.reshape(1, -1),
        tokens,
        route_ids.T,
        route_weights.T,
        moe_gain.reshape(-1, lanes),
        w_gate.reshape(w_gate.shape[1:]),
        w_up.reshape(w_up.shape[1:]),
        w_down.reshape(w_down.shape[1:]),
    )


def solution(mesh):
    in_specs = (
        P(("grp", "ep"), "tp"),
        P(("grp", "ep"), "tp"),
        P(("grp", "ep"), "tp"),
        P("tp"),
        P(),
        P(("grp", "ep"), None),
        P(("grp", "ep"), None),
        P(("grp", "ep"), None),
        P(),
        P("ep", None, "tp"),
        P("ep", None, "tp"),
        P("ep", "tp", None),
    )
    out_specs = (P(("grp", "ep"), "tp"), P(("grp", "ep"), "tp"))
    return jax.shard_map(
        on_device, mesh=mesh, in_specs=in_specs, out_specs=out_specs, check_vma=False
    )
```

```python
import functools

import jax
import jax.numpy as jnp
from jax import lax
from jax.experimental import pallas as pl
from jax.experimental.pallas import tpu as pltpu
from jax.sharding import PartitionSpec as P

MESH = pl.DeviceIdType.MESH
F32 = jnp.float32
BF16 = jnp.bfloat16
RIGHT, LEFT = 0, 1


def dot(a, b):
    return jnp.dot(a, b, preferred_element_type=F32)


def dot_nt(a, b):
    return lax.dot_general(a, b, (((1,), (1,)), ((), ())), preferred_element_type=F32)


def iota(shape, dim):
    return lax.broadcasted_iota(jnp.int32, shape, dim)


def kernel(
    E,
    T,
    q_hbm,
    k_hbm,
    v_hbm,
    lam_ref,
    hgain_hbm,
    tok_hbm,
    ids_hbm,
    rw_hbm,
    mgain_hbm,
    wg_hbm,
    wu_hbm,
    wd_hbm,
    heads_ref,
    eout_ref,
    q_s,
    hgain_s,
    tok_s,
    ids_s,
    rw_s,
    mgain_s,
    wg_s,
    wu_s,
    wd_s,
    normed_s,
    out_s,
    G,
    H,
    wts_a,
    wts_p,
    wts_q,
    dsend,
    drecv,
    res,
    back,
    Kb,
    Vb,
    scores,
    loc,
    joined,
    b_send,
    b_recv,
    x_send,
    x_recv,
    d_send,
    d_recv,
    e_send,
    e_recv,
    kv_send,
    kv_recv,
    sib_send,
    sib_recv,
):
    ep, tp = lax.axis_index("ep"), lax.axis_index("tp")
    nb = E // T
    Z = E // 2
    rows, width = tok_s.shape
    cap = out_s.shape[1]
    lanes = 128
    tail = cap // 2
    level = ep // 2

    x_to = (lax.rem(tp + 1, T), lax.rem(tp + T - 1, T))
    z_to = (lax.rem(ep + 2, E), lax.rem(ep + E - 2, E))
    sibling = ep + 1 - 2 * lax.rem(ep, 2)
    own_high = ep // T

    def partner(high, b):
        upper, under = high // 2, lax.rem(high, 2)
        upper = 1 - upper if b // 2 else upper
        under = 1 - under if b % 2 else under
        return 2 * upper + under

    def hops(b):
        return (T // 2, T // 2 - 1) if b % 2 == 0 else (T // 2 - 1, T // 2)

    near_first = sorted(range(nb), key=lambda b: (min(b, nb - b), b))
    far_first = near_first[::-1]

    barrier = pltpu.get_barrier_semaphore()

    def greet(i, _):
        @pl.when(i != ep)
        def _():
            pl.semaphore_signal(barrier, inc=1, device_id={"ep": i}, device_id_type=MESH)

        return 0

    lax.fori_loop(2 * level, E, greet, 0)
    for to in x_to:
        pl.semaphore_signal(barrier, inc=1, device_id={"tp": to}, device_id_type=MESH)

    local = [
        pltpu.make_async_copy(src, dst, loc.at[i])
        for i, (src, dst) in enumerate(
            (
                (ids_hbm, ids_s),
                (tok_hbm, tok_s),
                (mgain_hbm, mgain_s),
                (k_hbm, Kb.at[ep]),
                (v_hbm, Vb.at[ep]),
                (wg_hbm, wg_s),
                (wu_hbm, wu_s),
                (rw_hbm, rw_s),
                (wd_hbm, wd_s),
                (q_hbm, q_s),
                (hgain_hbm, hgain_s),
            )
        )
    ]
    c_ids, c_tok, c_mgain, c_k, c_v, c_wg, c_wu, c_rw, c_wd, c_q, c_hgain = local
    for copy in local:
        copy.start()

    pl.semaphore_wait(barrier, 2 * level + 3)

    def report(i, _):
        pl.semaphore_signal(joined.at[level], inc=1, device_id={"ep": i}, device_id_type=MESH)
        return 0

    lax.fori_loop(0, 2 * level, report, 0)

    def column(row):
        return jnp.transpose(jnp.broadcast_to(row, (lanes, rows)))

    c_ids.wait()
    ids = ids_s[...].astype(F32)
    id0, id1 = column(ids[0:1]), column(ids[1:2])
    lower = (iota((rows, rows), 1) < iota((rows, rows), 0)).astype(F32).astype(BF16)
    first = lax.rem(tp - lax.rem(ep, T) + T, T)
    lane = iota((rows, nb * cap), 1)
    lane_slot = lax.rem(lane, cap).astype(F32)
    lane_expert = (first + T * (lane // cap)).astype(F32)
    named = (id0 == lane_expert) | (id1 == lane_expert)
    earlier = dot(lower, named.astype(F32).astype(BF16))
    chosen = jnp.where(named & (earlier == lane_slot), 1.0, 0.0)
    select = jnp.transpose(chosen).astype(BF16)

    c_tok.wait()
    c_mgain.wait()
    gain = jnp.concatenate([mgain_s[i : i + 1] for i in range(width // lanes)], axis=1)
    step_rows = 32

    def norm(i, _):
        at = pl.ds(pl.multiple_of(i * step_rows, step_rows), step_rows)
        x = tok_s[at, :].astype(F32)
        scale = lax.rsqrt(jnp.mean(x * x, axis=1, keepdims=True) + 1e-06)
        normed_s[at, :] = (x * scale * gain).astype(BF16)
        return 0

    lax.fori_loop(0, rows // step_rows, norm, 0)
    out_s[...] = dot(select, normed_s[...]).astype(BF16).reshape(nb, cap, width)

    def dispatch(q):
        return pltpu.make_async_remote_copy(
            src_ref=out_s.at[q],
            dst_ref=G.at[own_high, tp],
            send_sem=b_send.at[q],
            recv_sem=b_recv.at[own_high],
            device_id={"ep": first + T * q},
            device_id_type=MESH,
        )

    def arrived(g):
        return pltpu.make_async_copy(G.at[g, tp], G.at[g, tp], b_recv.at[g])

    for k in range(nb):
        q = partner(own_high, k)
        expert = first + T * q

        @pl.when((expert // 2 <= level) & (expert != ep))
        def _():
            dispatch(q).start()

        @pl.when(expert == ep)
        def _():
            pltpu.make_async_copy(out_s.at[q], G.at[own_high, tp], b_recv.at[own_high]).start()

    def later(z, _):
        pl.semaphore_wait(joined.at[z], 2)
        q = z // (T // 2)

        @pl.when((first + T * q) // 2 == z)
        def _():
            dispatch(q).start()

        return 0

    lax.fori_loop(level + 1, Z, later, 0)

    buffers = (Kb, Vb)
    kv_hops = ((Z // 2, Z // 2 - 1), (Z // 2 - 1, Z // 2))

    def kv_copy(which, way, step):
        origin = lax.rem(ep + (2 * step if way == LEFT else 2 * E - 2 * step), E)
        return pltpu.make_async_remote_copy(
            src_ref=buffers[which].at[origin],
            dst_ref=buffers[which].at[origin],
            send_sem=kv_send,
            recv_sem=kv_recv.at[which, way, step],
            device_id={"ep": z_to[way]},
            device_id_type=MESH,
        )

    def sib_copy(which, way, step):
        origin = lax.rem(ep + (2 * step if way == LEFT else 2 * E - 2 * step), E)
        return pltpu.make_async_remote_copy(
            src_ref=buffers[which].at[origin],
            dst_ref=buffers[which].at[origin],
            send_sem=sib_send.at[which],
            recv_sem=sib_recv.at[which],
            device_id={"ep": sibling},
            device_id_type=MESH,
        )

    def kv_start():
        c_k.wait()
        c_v.wait()
        for which in (0, 1):
            kv_copy(which, RIGHT, 0).start()
            kv_copy(which, LEFT, 0).start()
            sib_copy(which, RIGHT, 0).start()

    def kv_step(s):
        for which in (0, 1):
            for way in (RIGHT, LEFT):
                if s <= kv_hops[which][way]:
                    kv_copy(which, way, s - 1).wait_recv()
                    if s < kv_hops[which][way]:
                        kv_copy(which, way, s).start()
                    sib_copy(which, way, s).start()

    half = T // 2
    pair_count = 2
    size = nb // pair_count

    def group(k):
        return partner(own_high, k)

    def ring_copy(k, way, step):
        origin = lax.rem(tp + (step if way == LEFT else T - step), T)
        return pltpu.make_async_remote_copy(
            src_ref=G.at[group(k), origin],
            dst_ref=G.at[group(k), origin],
            send_sem=x_send,
            recv_sem=x_recv.at[way, k, step],
            device_id={"tp": x_to[way]},
            device_id_type=MESH,
        )

    def hidden_of(p, origins):
        places = [(group(k), o) for k in range(p * size, (p + 1) * size) for o in origins]
        x = jnp.concatenate([G[g, o] for g, o in places], axis=0)
        gate = dot(x, wg_s[...])
        up = dot(x, wu_s[...])
        hidden = (gate / (1.0 + jnp.exp(-gate)) * up).astype(BF16)
        for i, (g, o) in enumerate(places):
            H[g, o] = hidden[i * cap : (i + 1) * cap]

    def combine_weights():
        c_rw.wait()
        w0, w1 = column(rw_s[0:1, :]), column(rw_s[1:2, :])
        lane_e = iota((rows, lanes), 1).astype(F32)
        hit0, hit1 = id0 == lane_e, id1 == lane_e
        before = dot(lower, jnp.where(hit0 | hit1, 1.0, 0.0).astype(BF16))
        pos0 = jnp.sum(jnp.where(hit0, before, 0.0), axis=1, keepdims=True)
        pos1 = jnp.sum(jnp.where(hit1, before, 0.0), axis=1, keepdims=True)
        nowhere = -1.0

        def fill(ref, slot0, slot1):
            columns = ref.shape[2]

            def tile(i, _):
                at = pl.ds(pl.multiple_of(i * lanes, lanes), lanes)
                here = (iota((rows, lanes), 1) + i * lanes).astype(F32)
                w = jnp.where(here == slot0, w0, 0.0) + jnp.where(here == slot1, w1, 0.0)
                high = w.astype(BF16)
                ref[0, :, at] = high
                ref[1, :, at] = (w - high.astype(F32)).astype(BF16)
                return 0

            lax.fori_loop(0, columns // lanes, tile, 0)

        fill(wts_a, id0 * cap + pos0, id1 * cap + pos1)
        fill(
            wts_p,
            jnp.where(pos0 < tail, id0 * tail + pos0, nowhere),
            jnp.where(pos1 < tail, id1 * tail + pos1, nowhere),
        )
        fill(
            wts_q,
            jnp.where(pos0 >= tail, id0 * tail + pos0 - tail, nowhere),
            jnp.where(pos1 >= tail, id1 * tail + pos1 - tail, nowhere),
        )

    def own_part(target, b):
        pair, odd = target // 2, lax.rem(target, 2)
        h = H[partner(own_high, b)].reshape(T * cap, H.shape[3])
        wa = wd_s[:, pl.ds(pl.multiple_of((3 * pair + 2 * odd) * lanes, lanes), lanes)]
        wb = wd_s[:, pl.ds(pl.multiple_of((3 * pair + 1) * lanes, lanes), lanes)]
        a = dot(h, wa).reshape(T, cap, lanes)
        m = dot(h, wb)
        m = jnp.where(odd == 1, pltpu.roll(m, lanes // 2, 1), m)
        r = pltpu.roll(m, lanes // 2, 1).reshape(T, cap, lanes)[:, tail:]
        m = m.reshape(T, cap, lanes)[:, :tail]
        low = iota((T, tail, lanes), 2) < lanes // 2
        return a, jnp.where(low, m, r)

    def place(b, way, step):
        return b * (T - 1) + (hops(b)[RIGHT] if way == LEFT else 0) + step

    def partial_copy(b, way, step):
        return pltpu.make_async_remote_copy(
            src_ref=dsend.at[place(b, way, step)],
            dst_ref=drecv.at[way, b, step],
            send_sem=d_send,
            recv_sem=d_recv.at[way, b, step],
            device_id={"tp": x_to[way]},
            device_id_type=MESH,
        )

    def own_for(b, way, step):
        left_to_go = hops(b)[way] - step
        target = lax.rem(tp + (left_to_go if way == RIGHT else T - left_to_go), T)
        return own_part(target, b)

    def pass_on(b, way, step, a, m):
        if step > 0:
            partial_copy(b, way, step - 1).wait_recv()
            a = a + drecv[way, b, step - 1, :, :cap].astype(F32)
            m = m + drecv[way, b, step - 1, :, cap:].astype(F32)
        dsend[place(b, way, step), :, :cap] = a.astype(BF16)
        dsend[place(b, way, step), :, cap:] = m.astype(BF16)
        partial_copy(b, way, step).start()

    def source_of(b, j):
        return lax.rem(j + T - lax.rem(ep, T), T) + T * partner(own_high, b)

    def send_back(b, j):
        return pltpu.make_async_remote_copy(
            src_ref=res.at[b, j],
            dst_ref=back.at[ep],
            send_sem=e_send,
            recv_sem=e_recv.at[own_high],
            device_id={"ep": source_of(b, j)},
            device_id_type=MESH,
        )

    def finish(b, a, m):
        for way in (RIGHT, LEFT):
            last = hops(b)[way] - 1
            partial_copy(b, way, last).wait_recv()
            a = a + drecv[way, b, last, :, :cap].astype(F32)
            m = m + drecv[way, b, last, :, cap:].astype(F32)
        res[b, :, :cap] = a.astype(BF16)
        res[b, :, cap:] = m.astype(BF16)

        def send(j, _):
            @pl.when(source_of(b, j) != ep)
            def _():
                send_back(b, j).start()

            @pl.when(source_of(b, j) == ep)
            def _():
                pltpu.make_async_copy(res.at[b, j], back.at[ep], e_recv.at[own_high]).start()

            return 0

        lax.fori_loop(0, T, send, 0)

    keys = Kb.shape[1]
    span = 4

    def attend():
        q = q_s[...].astype(F32) * (lanes // 2) ** -0.5
        first_half = iota(q.shape, 1) < lanes // 2
        q = jnp.concatenate([jnp.where(first_half, q, 0.0), jnp.where(first_half, 0.0, q)], axis=0)
        q = q.astype(BF16)
        top = jnp.full((2 * keys, keys), -jnp.inf, F32)
        for i in range(E // span):
            k = Kb[i * span : (i + 1) * span].reshape(span * keys, lanes)
            s = dot_nt(q, k)
            scores[:, i * span * keys : (i + 1) * span * keys] = s
            for g in range(span):
                top = jnp.maximum(top, s[:, g * keys : (g + 1) * keys])
        top = jnp.max(top, axis=1, keepdims=True)
        means = []
        for c in range(2):
            at_rows = slice(c * keys, (c + 1) * keys)
            high = jnp.broadcast_to(top[at_rows], (keys, span * keys))
            total = jnp.zeros((keys, keys), F32)
            sums = jnp.zeros((keys, lanes), F32)
            for i in range(E // span):
                w = jnp.exp(scores[at_rows, i * span * keys : (i + 1) * span * keys] - high)
                for g in range(span):
                    total = total + w[:, g * keys : (g + 1) * keys]
                v = Vb[i * span : (i + 1) * span].reshape(span * keys, lanes)
                sums = sums + dot(w.astype(BF16), v)
            means.append(sums / jnp.sum(total, axis=1, keepdims=True))
        return means

    kv_left = list(range(1, Z // 2 + 1))
    begin = {2: half + 1, 3: half + 1, 1: half, 0: half + 3}
    for slot in range(max(begin.values()) + half + 1):
        for p in range(pair_count):
            s = slot - p
            if s < 0 or s > half:
                continue
            for k in range(p * size, (p + 1) * size):
                if s == 0:
                    arrived(group(k)).wait()
                for way in (RIGHT, LEFT):
                    if 0 < s <= hops(k)[way]:
                        ring_copy(k, way, s - 1).wait_recv()
                    if s < hops(k)[way]:
                        ring_copy(k, way, s).start()
            if slot == 0:
                kv_start()
                combine_weights()
                c_wg.wait()
                c_wu.wait()
            if s == 0 or s == half:
                hidden_of(p, [lax.rem(tp + s, T)])
            else:
                hidden_of(p, [lax.rem(tp + T - s, T), lax.rem(tp + s, T)])
        if slot == half:
            c_wd.wait()
        work = []
        for b in begin:
            step = slot - begin[b]
            if 0 <= step < half:
                ways = [way for way in (RIGHT, LEFT) if step < hops(b)[way]]
                work.extend((b, way, step, *own_for(b, way, step)) for way in ways)
            if step == half:
                work.append((b, None, step, *own_part(tp, b)))
        for b, way, step, a, m in work:
            if way is None:
                finish(b, a, m)
            else:
                pass_on(b, way, step, a, m)
        if slot > 0 and kv_left:
            kv_step(kv_left.pop(0))

    for which in (0, 1):
        pltpu.make_async_copy(
            buffers[which].at[pl.ds(0, Z)], buffers[which].at[pl.ds(0, Z)], sib_recv.at[which]
        ).wait()
    c_q.wait()
    c_hgain.wait()
    mean0, mean1 = attend()
    mixed = mean0 - lam_ref[0] * mean1
    scale = lax.rsqrt(jnp.mean(mixed * mixed, axis=1, keepdims=True) + 1e-06)
    heads_ref[...] = (mixed * scale * hgain_s[...]).astype(BF16)

    def quarter(b, carry):
        high = partner(own_high, b)
        part = back.at[pl.ds(high * T, T)]
        pltpu.make_async_copy(part, part, e_recv.at[high]).wait()
        wide = part[:, :cap, :].reshape(T * cap, lanes)
        packed = part[:, cap:, :].reshape(T * tail, lanes)
        at = pl.ds(pl.multiple_of(high * T * cap, lanes), T * cap)
        at_tail = pl.ds(pl.multiple_of(high * T * tail, lanes), T * tail)
        a, m, n = carry
        a = a + dot(wts_a[0, :, at], wide) + dot(wts_a[1, :, at], wide)
        m = m + dot(wts_p[0, :, at_tail], packed) + dot(wts_p[1, :, at_tail], packed)
        n = n + dot(wts_q[0, :, at_tail], packed) + dot(wts_q[1, :, at_tail], packed)
        return a, m, n

    carry = (jnp.zeros((rows, lanes), F32),) * 3
    for b in far_first:
        carry = quarter(b, carry)
    a, m, n = carry
    m = m + pltpu.roll(n, lanes // 2, 1)
    turned = pltpu.roll(a, lanes // 2, 1)
    low = iota(a.shape, 1) < lanes // 2
    odd = lax.rem(tp, 2) == 1
    eout_ref[:, :lanes] = jnp.where(odd, jnp.where(low, m, turned), a).astype(BF16)
    rest = jnp.where(odd, turned, m).astype(BF16)
    eout_ref[:, lanes:] = rest[:, : lanes // 2]

    for b in range(nb):

        @pl.when(first + T * b != ep)
        def _():
            dispatch(b).wait_send()

    pltpu.make_async_copy(dsend, dsend, x_send).wait()
    pltpu.make_async_copy(dsend, dsend, d_send).wait()
    pltpu.make_async_copy(Kb.at[pl.ds(0, E - 2)], Kb.at[pl.ds(0, E - 2)], kv_send).wait()
    for which in (0, 1):
        pltpu.make_async_copy(
            buffers[which].at[pl.ds(0, Z)], buffers[which].at[pl.ds(0, Z)], sib_send.at[which]
        ).wait()
    pltpu.make_async_copy(back.at[pl.ds(0, E - 1)], back.at[pl.ds(0, E - 1)], e_send).wait()


def on_device(
    queries,
    keys,
    values,
    lambdas,
    head_gain,
    tokens,
    route_ids,
    route_weights,
    moe_gain,
    w_gate,
    w_up,
    w_down,
):
    E, T = lax.axis_size("ep"), lax.axis_size("tp")
    nb, Z = E // T, E // 2
    rows, width = tokens.shape
    cap = 2 * rows * route_ids.shape[1] // E
    q_rows, lanes = queries.shape
    units = w_gate.shape[2]
    slice_width = width // T
    block_rows = cap * slice_width // lanes
    half = T // 2
    dma = pltpu.SemaphoreType.DMA
    anywhere = pl.BlockSpec(memory_space=pltpu.HBM)
    scratch = [
        pltpu.VMEM((q_rows, lanes), BF16),
        pltpu.VMEM((1, lanes), F32),
        pltpu.VMEM((rows, width), BF16),
        pltpu.VMEM(route_ids.shape[::-1], jnp.int32),
        pltpu.VMEM(route_weights.shape[::-1], F32),
        pltpu.VMEM((width // lanes, lanes), F32),
        pltpu.VMEM((width, units), BF16),
        pltpu.VMEM((width, units), BF16),
        pltpu.VMEM((units, width), BF16),
        pltpu.VMEM((rows, width), BF16),
        pltpu.VMEM((nb, cap, width), BF16),
        pltpu.VMEM((nb, T, cap, width), BF16),
        pltpu.VMEM((nb, T, cap, units), BF16),
        pltpu.VMEM((2, rows, E * cap), BF16),
        pltpu.VMEM((2, rows, E * cap // 2), BF16),
        pltpu.VMEM((2, rows, E * cap // 2), BF16),
        pltpu.VMEM((nb * (T - 1), T, block_rows, lanes), BF16),
        pltpu.VMEM((2, nb, half, T, block_rows, lanes), BF16),
        pltpu.VMEM((nb, T, block_rows, lanes), BF16),
        pltpu.VMEM((E, block_rows, lanes), BF16),
        pltpu.VMEM((E, q_rows, lanes), BF16),
        pltpu.VMEM((E, q_rows, lanes), BF16),
        pltpu.VMEM((2 * q_rows, E * q_rows), F32),
        dma((11,)),
        pltpu.SemaphoreType.REGULAR((Z,)),
        dma((nb,)),
        dma((nb,)),
        dma,
        dma((2, nb, half)),
        dma,
        dma((2, nb, half)),
        dma,
        dma((nb,)),
        dma,
        dma((2, 2, Z // 2)),
        dma((2,)),
        dma((2,)),
    ]
    return pl.pallas_call(
        functools.partial(kernel, E, T),
        out_shape=(
            jax.ShapeDtypeStruct((q_rows, lanes), BF16),
            jax.ShapeDtypeStruct((rows, slice_width), BF16),
        ),
        in_specs=[anywhere] * 3
        + [pl.BlockSpec(memory_space=pltpu.SMEM)]
        + [anywhere] * 8,
        out_specs=(pl.BlockSpec(memory_space=pltpu.VMEM),) * 2,
        scratch_shapes=scratch,
        compiler_params=pltpu.CompilerParams(
            collective_id=0, has_side_effects=True, vmem_limit_bytes=62 * 1024 * 1024
        ),
    )(
        queries,
        keys,
        values,
        lambdas,
        head_gain.reshape(1, -1),
        tokens,
        route_ids.T,
        route_weights.T,
        moe_gain.reshape(-1, lanes),
        w_gate.reshape(w_gate.shape[1:]),
        w_up.reshape(w_up.shape[1:]),
        w_down.reshape(w_down.shape[1:]),
    )


def solution(mesh):
    in_specs = (
        P(("grp", "ep"), "tp"),
        P(("grp", "ep"), "tp"),
        P(("grp", "ep"), "tp"),
        P("tp"),
        P(),
        P(("grp", "ep"), None),
        P(("grp", "ep"), None),
        P(("grp", "ep"), None),
        P(),
        P("ep", None, "tp"),
        P("ep", None, "tp"),
        P("ep", "tp", None),
    )
    out_specs = (P(("grp", "ep"), "tp"), P(("grp", "ep"), "tp"))
    return jax.shard_map(
        on_device, mesh=mesh, in_specs=in_specs, out_specs=out_specs, check_vma=False
    )
```
